32 devices in a mesh: sp: 4 (over y, x), tp: 8 (over z, core).
Axes of the slice: x: 2, y: 2, z: 4, core: 2. Of those that a mesh axis runs over, the one named last changes fastest.
Arguments:
- layer_input: bfloat16 [2048, 2048], P(('sp', 'tp')), may hold values from -6 to 6
- receptance: bfloat16 [2048, 2048], P('sp', 'tp'), may hold values from -6 to 6
- keys: bfloat16 [2048, 2048], P('sp', 'tp'), may hold values from -6 to 6
- values: bfloat16 [2048, 2048], P('sp', 'tp'), may hold values from -6 to 6
- erase_preact: bfloat16 [2048, 2048], P('sp', 'tp'), may hold values from -12 to 5
- decay_preact: bfloat16 [2048, 2048], P('sp', 'tp'), may hold values from -40 to 3
- decay_spike: float32 [2048, 32], P('sp', 'tp'), may hold values from -2 to 0
- head_norm_gain: bfloat16 [2048], P('tp'), may hold values from 0.099609375 to 1.8984375
- output_weight: bfloat16 [2048, 2048], P('tp'), may hold values from -0.125 to 0.125
- expert_norm_gain: bfloat16 [2048], replicated, may hold values from 0.099609375 to 1.8984375
- routes: int32 [2048, 2], P(('sp', 'tp')), may hold values from 0 to 7, all different within a row; in each aligned block of 64 rows (0 to 63, 64 to 127, ...) at most 24 rows name the same one
- routing_weight: float32 [2048, 2], P(('sp', 'tp')), may hold values from 0.3 to 1.5
- expert_gate_weight: bfloat16 [8, 2048, 4096], P('sp', None, 'tp'), may hold values from -0.125 to 0.125
- expert_up_weight: bfloat16 [8, 2048, 4096], P('sp', None, 'tp'), may hold values from -0.125 to 0.125
- expert_down_weight: bfloat16 [8, 4096, 2048], P('sp', 'tp'), may hold values from -0.09375 to 0.09375
- shared_gate_weight: bfloat16 [2048, 4096], P(None, 'tp'), may hold values from -0.125 to 0.125
- shared_up_weight: bfloat16 [2048, 4096], P(None, 'tp'), may hold values from -0.125 to 0.125
- shared_down_weight: bfloat16 [4096, 2048], P('tp'), may hold values from -0.09375 to 0.09375
Outputs:
- layer_out: bfloat16 [2048, 2048], P(('sp', 'tp'))
The draws below stay inside these ranges and needn't reach their ends.
Inputs may be any that keep to these rules, and one draw needn't show every extreme that they name: `routes`: in each aligned block of 64 rows no expert is named by more than 24 rows.
All inputs are finite; a program needn't handle non-finite values.
Results may differ from the reference program's by a relative error of at most 0.02.
Values may be sent and summed in bfloat16 or wider, within the bound.
A program may use at most 128 MiB of HBM per device.

```python
import math
import jax
import jax.numpy as jnp
import numpy as np
from jax import lax

D = 2048
HEAD = 64
HEADS = 32
TOK_DEV = 512
TOKENS = 2048
ROWS_DEV = 64
EXPERTS = 8
TOP_K = 2
FFE = 4096
SH = 4096
CAP = 24
N_SP = 4
N_TP = 8


def slow_heads(key):
    slow_count = HEADS // 2
    order = jax.random.permutation(jax.random.fold_in(key, 41), HEADS)
    return order < slow_count


def rough_noise(key, array_shape):
    return 0.8 * jax.random.truncated_normal(key, -3.0, 3.0, array_shape, jnp.float32)


def draw_keys(key, part):
    noise = jax.random.normal(jax.random.fold_in(key, 79), (TOKENS, D), jnp.float32)
    common = jax.random.normal(jax.random.fold_in(key, 73), (1, D), jnp.float32)
    return jnp.clip(common + noise, -6.0, 6.0).astype(jnp.bfloat16)


def draw_decay_preact(key, part):
    slow = slow_heads(key)
    fast_rate = jax.random.uniform(jax.random.fold_in(key, 43), (HEADS,), jnp.float32, 0.01, 0.033)
    head_rate = jnp.where(slow, 0.1 / TOKENS, fast_rate)
    head_base = jnp.repeat(jnp.log(head_rate) + 0.5, HEAD)[None, :]
    stretch = jax.random.uniform(jax.random.fold_in(key, 47), (TOKENS // TOK_DEV, 1), jnp.float32, -0.7, 0.7)
    per_block = jnp.repeat(stretch, TOK_DEV, axis=0)
    noise = rough_noise(jax.random.fold_in(key, 53), (TOKENS, D))
    return (head_base + per_block + noise).astype(jnp.bfloat16)


def draw_erase_preact(key, part):
    slow = slow_heads(key)
    fast_base = jax.random.uniform(jax.random.fold_in(key, 59), (HEADS,), jnp.float32, 2.0, 2.6)
    head_base = jnp.repeat(jnp.where(slow, -7.0, fast_base), HEAD)[None, :]
    noise = rough_noise(jax.random.fold_in(key, 61), (TOKENS, D))
    return jnp.clip(head_base + noise, -12.0, 5.0).astype(jnp.bfloat16)


def draw_decay_spike(key, part):
    where_hit = jax.random.randint(jax.random.fold_in(key, 67), (3,), 0, TOKENS)
    depth = jnp.log(jax.random.uniform(jax.random.fold_in(key, 71), (3, HEADS), jnp.float32, 0.5, 0.8))
    hits = (jnp.arange(TOKENS, dtype=jnp.int32)[:, None] == where_hit[None, :]).astype(jnp.float32)
    return jnp.dot(hits, depth)


def levels(rng, shape, split, low, largest):
    def one(dim, blocks):
        steps = jax.random.uniform(jax.random.fold_in(jax.random.fold_in(rng, 6), dim), (blocks,), jnp.float32, low / len(split), largest / len(split))
        return jnp.repeat(jnp.exp(steps), shape[dim] // blocks).reshape((-1,) + (1,) * (len(shape) - dim - 1))

    factor_of = one(*split[0])
    for cut in split[1:]:
        factor_of = factor_of * one(*cut)
    return factor_of


def routed_block(key, own, number, rows, amount, top, bound, skew):
    sequence = jax.random.permutation(key, amount)
    packed, ordinary = shares(amount, rows * top, bound, skew, True), shares(amount, rows * top, bound, skew, False)
    places = jnp.arange(amount)

    def named(sizes, turn):
        used = int((sizes > 0).sum())
        fixed = max(1, used // 4)
        shifted = fixed + (places - fixed + turn * (used - fixed)) % max(1, amount - fixed)
        return jnp.zeros((amount,), jnp.int32).at[sequence[jnp.where(places < fixed, places, shifted)]].set(jnp.asarray(sizes, jnp.int32))

    sizes = jnp.where(number % 4 == 0, named(packed, number // 4), named(ordinary, number - number // 4 - 1))
    mixed = jax.random.permutation(jax.random.fold_in(own, 3), amount)
    giver, taker = mixed[0:amount // 2 * 2:2], mixed[1:amount // 2 * 2:2]
    margin = jnp.minimum(sizes[giver] - 1, bound - sizes[taker]) // 2
    margin = jnp.where((giver == sequence[0]) | (taker == sequence[0]) | (sizes[taker] == 0), 0, jnp.maximum(margin, 0))
    shifted = jax.random.randint(jax.random.fold_in(own, 4), (amount // 2,), 0, 1 << 20) % (margin + 1)
    sizes = sizes.at[giver].add(-shifted).at[taker].add(shifted)
    members = jnp.searchsorted(jnp.cumsum(sizes), jnp.arange(rows * top), side="right").astype(jnp.int32)
    table = members.reshape(top, rows).T
    table = table[jax.random.permutation(jax.random.fold_in(own, 1), rows)]
    turn = jax.random.randint(jax.random.fold_in(own, 2), (rows, 1), 0, top)
    return jnp.take_along_axis(table, (jnp.arange(top)[None, :] + turn) % top, axis=1)


def shares(number_of, total, bound, skew, full):
    loads = [(1 << 20) // math.isqrt(standing ** skew) + 1 for standing in range(1, number_of + 1)]
    largest = bound if full else min(bound, max(-(-total // number_of), total * loads[0] // sum(loads)))
    least = 1 if total - largest >= number_of - 1 else 0
    given, surplus = [largest] + [least] * (number_of - 1), total - largest - least * (number_of - 1)
    while surplus > 0:
        free = [i for i in range(1, number_of) if given[i] < largest] or [i for i in range(1, number_of) if given[i] < bound]
        pool, remaining = sum([loads[i] for i in free]), surplus
        for i in free:
            extra = min(bound - given[i], max(1, remaining * loads[i] // pool), surplus)
            given[i] = given[i] + extra
            surplus = surplus - extra
    return np.array(given)


def bell_draw(rng, dims, scale, reach, cuts=(), kind=jnp.bfloat16):
    factor_of = levels(rng, dims, cuts, -0.22, 0.18) if cuts else 1.0
    drawn = jax.random.normal(rng, dims, jnp.float32) * scale * factor_of
    return jnp.minimum(jnp.maximum(drawn, -reach), reach).astype(kind)


def setup_inputs(seed: int = 0) -> dict:
    key_list = jax.random.split(jax.random.key(seed), 19)
    layer_input = bell_draw(key_list[0], (TOKENS, D), 1.0, 6.0, ((0, 32),))
    receptance = bell_draw(key_list[1], (TOKENS, D), 1.0, 6.0, ((0, 4), (1, 8)))
    keys = draw_keys(jax.random.fold_in(key_list[18], 71), 0)
    values = bell_draw(key_list[3], (TOKENS, D), 1.0, 6.0, ((0, 4), (1, 8)))
    erase_preact = draw_erase_preact(jax.random.fold_in(key_list[18], 71), 0)
    decay_preact = draw_decay_preact(jax.random.fold_in(key_list[18], 71), 0)
    decay_spike = draw_decay_spike(jax.random.fold_in(key_list[18], 71), 0)
    head_norm_gain = jnp.clip(1.0 + 0.18 * jax.random.normal(key_list[7], (D,), jnp.float32), 0.099609375, 1.8984375).astype(jnp.bfloat16)
    output_weight = bell_draw(key_list[8], (D, D), D ** -0.5, 0.125, ((0, 8),))
    expert_norm_gain = jnp.clip(1.0 + 0.18 * jax.random.normal(key_list[9], (D,), jnp.float32), 0.099609375, 1.8984375).astype(jnp.bfloat16)
    routes_keys = jax.random.split(jax.random.fold_in(key_list[10], 1), TOKENS // ROWS_DEV)
    routes_turns = jax.random.permutation(jax.random.fold_in(key_list[10], 3), TOKENS // ROWS_DEV)
    routes = jax.vmap(lambda own, number: routed_block(jax.random.fold_in(key_list[10], 2), own, number, ROWS_DEV, EXPERTS, TOP_K, CAP, 2))(routes_keys, routes_turns).reshape((TOKENS, TOP_K))
    routing_weight = jnp.clip(0.3 + 1.2 * jax.random.uniform(key_list[11], (TOKENS, TOP_K), jnp.float32) ** levels(key_list[11], (TOKENS, TOP_K), ((0, 32),), -0.2, 0.2), 0.3, 1.5)
    expert_gate_weight = bell_draw(key_list[12], (EXPERTS, D, FFE), D ** -0.5, 0.125, ((0, 4), (2, 8)))
    expert_up_weight = bell_draw(key_list[13], (EXPERTS, D, FFE), D ** -0.5, 0.125, ((0, 4), (2, 8)))
    expert_down_weight = bell_draw(key_list[14], (EXPERTS, FFE, D), FFE ** -0.5, 0.09375, ((0, 4), (1, 8)))
    shared_gate_weight = bell_draw(key_list[15], (D, SH), D ** -0.5, 0.125, ((1, 8),))
    shared_up_weight = bell_draw(key_list[16], (D, SH), D ** -0.5, 0.125, ((1, 8),))
    shared_down_weight = bell_draw(key_list[17], (SH, D), SH ** -0.5, 0.09375, ((0, 8),))
    return dict(layer_input=layer_input, receptance=receptance, keys=keys, values=values, erase_preact=erase_preact, decay_preact=decay_preact, decay_spike=decay_spike, head_norm_gain=head_norm_gain, output_weight=output_weight, expert_norm_gain=expert_norm_gain, routes=routes, routing_weight=routing_weight, expert_gate_weight=expert_gate_weight, expert_up_weight=expert_up_weight, expert_down_weight=expert_down_weight, shared_gate_weight=shared_gate_weight, shared_up_weight=shared_up_weight, shared_down_weight=shared_down_weight)


highest = lax.Precision.HIGHEST
GN_EPS = 0.00064
RMS_EPS = 1e-06

def each_head(array):
    return array.astype(jnp.float32).reshape(array.shape[0], HEADS, HEAD)

def recurrence(decay_factor, unit_keys, beta, key_rows, value_rows, read_rows):

    def advance(state_now, inputs):
        decay_t, unit_t, beta_t, key_t, value_t, read_t = inputs
        removed = jnp.einsum('hij,hj->hi', state_now, unit_t, precision=highest)
        state_now = state_now * decay_t[:, None, :] - removed[:, :, None] * beta_t[:, None, :] + value_t[:, :, None] * key_t[:, None, :]
        return (state_now, jnp.einsum('hij,hj->hi', state_now, read_t, precision=highest))
    start_state = jnp.zeros((HEADS, HEAD, HEAD), jnp.float32)
    _, outputs = lax.scan(advance, start_state, (decay_factor, unit_keys, beta, key_rows, value_rows, read_rows))
    return outputs

def grouped_down(hidden, down, groups):
    group_cols = hidden.shape[1] // groups

    def add_group(running, group_idx):
        first_col = (group_idx * group_cols).astype(jnp.int32)
        hidden_part = lax.dynamic_slice_in_dim(hidden, first_col, group_cols, 1)
        down_part = lax.dynamic_slice_in_dim(down, first_col, group_cols, 0)
        partial_value = jnp.dot(hidden_part, down_part, preferred_element_type=jnp.float32).astype(jnp.bfloat16)
        partial_value = lax.optimization_barrier(partial_value)
        return (running + partial_value.astype(jnp.float32), None)
    running, _ = lax.scan(add_group, jnp.zeros((hidden.shape[0], down.shape[1]), jnp.float32), jnp.arange(groups, dtype=jnp.int32))
    return running

def reference(layer_input, receptance, keys, values, erase_preact, decay_preact, decay_spike, head_norm_gain, output_weight, expert_norm_gain, routes, routing_weight, expert_gate_weight, expert_up_weight, expert_down_weight, shared_gate_weight, shared_up_weight, shared_down_weight):
    key_rows = each_head(keys)
    unit_keys = key_rows * lax.rsqrt(lax.optimization_barrier(jnp.sum(key_rows * key_rows, axis=-1, keepdims=True)) + 1e-06)
    beta = unit_keys * jax.nn.sigmoid(each_head(erase_preact))
    decay_factor = jnp.exp(-jnp.exp(-jax.nn.softplus(-each_head(decay_preact)) - 0.5) + decay_spike.astype(jnp.float32)[:, :, None])
    value_rows = each_head(values)
    read_rows = each_head(receptance)
    forward = recurrence(decay_factor, unit_keys, beta, key_rows, value_rows, read_rows)
    flipped = [array[::-1] for array in (decay_factor, unit_keys, beta, key_rows, value_rows, read_rows)]
    backward = recurrence(*flipped)[::-1]
    mix = forward + backward
    center = lax.optimization_barrier(jnp.mean(mix, axis=-1, keepdims=True))
    spread = lax.optimization_barrier(jnp.mean(jnp.square(mix - center), axis=-1, keepdims=True))
    mixed = ((mix - center) * lax.rsqrt(spread + GN_EPS)).reshape(TOKENS, D) * head_norm_gain.astype(jnp.float32)
    mixed = mixed.astype(jnp.bfloat16)
    residual = layer_input.astype(jnp.float32) + jnp.dot(mixed, output_weight, preferred_element_type=jnp.float32)
    normed = residual * lax.rsqrt(lax.optimization_barrier(jnp.mean(residual * residual, axis=-1, keepdims=True)) + RMS_EPS)
    normed = (normed * expert_norm_gain.astype(jnp.float32)).astype(jnp.bfloat16)
    shared_hidden = (jax.nn.silu(jnp.dot(normed, shared_gate_weight, preferred_element_type=jnp.float32)) * jnp.dot(normed, shared_up_weight, preferred_element_type=jnp.float32)).astype(jnp.bfloat16)
    shared = grouped_down(shared_hidden, shared_down_weight, N_TP)
    entries = routes.reshape(-1).astype(jnp.int32)
    entry_weight = routing_weight.reshape(-1).astype(jnp.float32)
    entry_owner = jnp.arange(TOKENS * TOP_K, dtype=jnp.int32) // TOP_K
    most_rows = N_SP * N_TP * CAP

    def one_expert(running, expert):
        chosen = entries == expert
        position = jnp.cumsum(chosen.astype(jnp.int32)) - 1
        target = jnp.where(chosen, position, most_rows).astype(jnp.int32)
        owners = jnp.full((most_rows,), TOKENS, jnp.int32).at[target].set(entry_owner, mode='drop')
        weights = jnp.zeros((most_rows,), jnp.float32).at[target].set(entry_weight, mode='drop')
        picked = jnp.take(normed, jnp.minimum(owners, TOKENS - 1).astype(jnp.int32), axis=0)
        gate_value = jnp.dot(picked, expert_gate_weight[expert], preferred_element_type=jnp.float32)
        up_value = jnp.dot(picked, expert_up_weight[expert], preferred_element_type=jnp.float32)
        hidden = (jax.nn.silu(gate_value) * up_value).astype(jnp.bfloat16)
        routed = grouped_down(hidden, expert_down_weight[expert], N_TP).astype(jnp.bfloat16)
        routed = lax.optimization_barrier(routed)
        running = running.at[owners].add(weights[:, None] * routed.astype(jnp.float32), mode='drop')
        return (running, None)
    routed_sum, _ = lax.scan(one_expert, jnp.zeros((TOKENS, D), jnp.float32), jnp.arange(EXPERTS, dtype=jnp.int32))
    return (residual + shared + routed_sum).astype(jnp.bfloat16)
```

```python
import functools
import jax
import jax.numpy as jnp
from jax import lax
from jax.experimental import pallas as pl
from jax.experimental.pallas import tpu as pltpu
from jax.sharding import PartitionSpec as P

SPAN = 64
GN_EPS = 0.00064
RMS_EPS = 1e-06
F32, BF16 = jnp.float32, jnp.bfloat16
MESH = pl.DeviceIdType.MESH
NN = (((1,), (0,)), ((), ()))
NT = (((1,), (1,)), ((), ()))
TN = (((0,), (0,)), ((), ()))


def mul(left, right, dims=NN):
    return lax.dot_general(left, right, dims, preferred_element_type=F32)


def halves(x):
    high = x.astype(BF16)
    return high, (x - high.astype(F32)).astype(BF16)


def product(left, right_high, right_low, dims=NN):
    rows = left.shape[0]
    high, low = halves(left)
    both = mul(jnp.concatenate([high, low], axis=0), right_high, dims)
    out = both[:rows] + both[rows:]
    if right_low is not None:
        out = out + mul(high, right_low, dims)
    return out


def mixer_kernel(
    geometry,
    r_ref, k_ref, v_ref, e_ref, dp_ref, spike_ref, gain_ref, w_ref, out_ref,
    local_s, readout_s, maps_s, prefix_s, send_maps, recv_maps,
    mixed_s, part_s, sib_s, summed_s, recv_s,
    map_send, map_recv, sib_send, sib_recv, z_send, z_recv,
):
    n_sp, n_tp, heads = geometry
    n_z = n_tp // 2
    tokens, wide = k_ref.shape
    width = wide // heads
    blocks = tokens // SPAN
    rows = tokens // n_tp
    sp, tp = lax.axis_index("sp"), lax.axis_index("tp")
    z, core = tp // 2, lax.rem(tp, 2)

    barrier = pltpu.get_barrier_semaphore()
    for d in range(1, n_sp):
        pl.semaphore_signal(barrier, inc=1, device_id=(lax.rem(sp + d, n_sp), tp), device_id_type=MESH)
    for d in range(1, n_z):
        pl.semaphore_signal(
            barrier, inc=1, device_id=(sp, lax.rem(z + d, n_z) * 2 + core), device_id_type=MESH
        )
    pl.semaphore_signal(barrier, inc=1, device_id=(sp, z * 2 + 1 - core), device_id_type=MESH)

    def head_mask(shape, dtype):
        first = lax.broadcasted_iota(jnp.int32, shape, 0) // width
        second = lax.broadcasted_iota(jnp.int32, shape, 1) // width
        return (first == second).astype(F32).astype(dtype)

    square = head_mask((wide, wide), BF16)

    def spread(x):
        return jnp.concatenate([x] * heads, axis=0) * square

    def spread_pair(x):
        high, low = halves(x)
        return spread(high), spread(low)

    def gather_heads(x):
        total = x[:width]
        for h in range(1, heads):
            total = total + x[h * width : (h + 1) * width]
        return total

    def lane_of(shape):
        return lax.broadcasted_iota(jnp.int32, shape, 1)

    row_t = lax.broadcasted_iota(jnp.int32, (SPAN, wide), 0)
    col_s = lax.rem(lane_of((SPAN, wide)), SPAN)
    below = row_t > col_s
    above = row_t < col_s
    same = row_t == col_s
    tri = (
        lax.broadcasted_iota(jnp.int32, (SPAN, SPAN), 0)
        >= lax.broadcasted_iota(jnp.int32, (SPAN, SPAN), 1)
    ).astype(F32).astype(BF16)
    tri3 = jnp.concatenate([tri, tri, tri], axis=1)
    eye = same.astype(F32)

    def each_block(b, carry):
        here = pl.ds(pl.multiple_of(b * SPAN, SPAN), SPAN)
        keys = k_ref[here, :].astype(F32)
        square_high, square_low = halves(keys * keys)
        norm = mul(jnp.concatenate([square_high, square_low], axis=0), square)
        norm = norm[:SPAN] + norm[SPAN:]
        unit = keys * lax.rsqrt(norm + 1e-06)
        beta = unit * jax.nn.sigmoid(e_ref[here, :].astype(F32))
        spikes = spike_ref[here, :]
        lane_head = lane_of((SPAN, wide)) // width
        spike = jnp.zeros((SPAN, wide), F32)
        for h in range(heads):
            spike = jnp.where(lane_head == h, spikes[:, h : h + 1], spike)
        decay = -0.6065306597126334 * jax.nn.sigmoid(dp_ref[here, :].astype(F32)) + spike
        decay_1 = decay.astype(BF16)
        rest = decay - decay_1.astype(F32)
        decay_2 = rest.astype(BF16)
        decay_3 = (rest - decay_2.astype(F32)).astype(BF16)
        cumulative = mul(tri3, jnp.concatenate([decay_1, decay_2, decay_3], axis=0))
        total = cumulative[SPAN - 1 : SPAN, :]
        middle = 0.5 * total
        e1 = jnp.exp(cumulative - middle)
        e2 = jnp.exp(cumulative - decay - middle)
        e3 = jnp.exp(middle - cumulative)
        e4 = jnp.exp(middle - cumulative + decay)
        em = jnp.exp(middle)
        et = jnp.exp(total)
        reads = r_ref[here, :].astype(F32)
        values = v_ref[here, :]
        value_wide = spread(values)
        local_sum = jnp.zeros((SPAN, wide), F32)
        for d in range(2):
            strict = below if d == 0 else above
            loose = strict | same
            left_scale, before_scale, right_scale = (e1, e2, e3) if d == 0 else (e4, e3, e2)
            left = jnp.concatenate([unit * before_scale, reads * left_scale], axis=0)
            beta_right = beta * right_scale
            key_right = keys * right_scale
            keep = jnp.concatenate([strict, loose], axis=0)
            from_beta = jnp.where(keep, product(left, *spread_pair(beta_right), dims=NT), 0.0)
            from_key = jnp.where(keep, product(left, *spread_pair(key_right), dims=NT), 0.0)
            key_part = product(from_key, value_wide, None)
            corner_all = from_beta[:SPAN]
            size, inverse = 1, None
            while size < SPAN:
                joined = row_t // (2 * size) == col_s // (2 * size)
                corner = jnp.where(joined & (row_t // size != col_s // size), corner_all, 0.0)
                if size == 1:
                    inverse = eye - corner
                else:
                    pair = spread_pair(inverse)
                    step = product(corner, *pair)
                    inverse = inverse - product(inverse, *spread_pair(step))
                size *= 2
            true_left = left * em
            solved_w = product(inverse, *spread_pair(true_left[:SPAN]))
            solved_v = product(inverse, *spread_pair(-key_part[:SPAN]))
            read = from_beta[SPAN:]
            local_sum = local_sum + key_part[SPAN:] + product(read, *spread_pair(solved_v))
            readout_s[d, here, :] = true_left[SPAN:] - product(read, *spread_pair(solved_w))
            beta_high, beta_low = halves(beta_right * em)
            key_high, key_low = halves(key_right * em)
            w_high, w_low = halves(solved_w)
            v_high, v_low = halves(solved_v)
            beta_three = [beta_high, beta_low, beta_high]
            move = mul(
                jnp.concatenate([w_high, w_high, w_low], axis=0),
                jnp.concatenate(beta_three, axis=0),
                TN,
            )
            put = mul(
                jnp.concatenate([v_high, v_high, v_low, values, values], axis=0),
                jnp.concatenate(beta_three + [key_high, key_low], axis=0),
                TN,
            )
            on_head = lax.broadcasted_iota(jnp.int32, (width, wide), 0) == lax.rem(
                lane_of((width, wide)), width
            )
            wide_mask = square.astype(F32)
            move = gather_heads(move * wide_mask)
            maps_s[d, b, :width, :] = jnp.where(on_head, et, 0.0) - move
            maps_s[d, b, width:, :] = gather_heads(put * wide_mask)
        local_s[here, :] = local_sum
        return carry

    lax.fori_loop(0, blocks, each_block, 0)

    first = (
        lax.broadcasted_iota(jnp.int32, (2 * width, wide), 0)
        == lax.rem(lane_of((2 * width, wide)), width)
    ).astype(F32)
    no_rows = jnp.zeros((width, wide), F32)

    def compose(i, carry):
        new = []
        for d in range(2):
            b = i if d == 0 else blocks - 1 - i
            prefix_s[d, b] = carry[d]
            moved = product(carry[d], *spread_pair(maps_s[d, b, :width, :]))
            new.append(moved + jnp.concatenate([no_rows, maps_s[d, b, width:, :]], axis=0))
        return tuple(new)

    whole = lax.fori_loop(0, blocks, compose, (first, first))
    for d in range(2):
        send_maps[d] = whole[d].astype(BF16)
    pl.semaphore_wait(barrier, n_sp - 1 + n_z)

    copies = []
    for d in range(1, n_sp):
        target = lax.rem(sp + d, n_sp)
        copy = pltpu.make_async_remote_copy(
            src_ref=send_maps.at[(target < sp).astype(jnp.int32)],
            dst_ref=recv_maps.at[sp],
            send_sem=map_send.at[d],
            recv_sem=map_recv.at[sp],
            device_id=(target, tp),
            device_id_type=MESH,
        )
        copy.start()
        copies.append(copy)
    for d in range(1, n_sp):
        source = lax.rem(sp + d, n_sp)
        pltpu.make_async_remote_copy(
            src_ref=send_maps.at[0],
            dst_ref=recv_maps.at[source],
            send_sem=map_send.at[d],
            recv_sem=map_recv.at[source],
            device_id=(source, tp),
            device_id_type=MESH,
        ).wait_recv()
    for copy in copies:
        copy.wait_send()
    recv_maps[sp] = jnp.zeros((2 * width, wide), BF16)

    def enter(i, carry):
        new = []
        for d in range(2):
            k = i if d == 0 else n_sp - 1 - i
            reached = (k < sp) if d == 0 else (k > sp)
            part = recv_maps[k]
            moved = product(carry[d], spread(part[:width]), None) + part[width:].astype(F32)
            new.append(jnp.where(reached, moved, carry[d]))
        return tuple(new)

    entry = lax.fori_loop(0, n_sp, enter, (no_rows, no_rows))

    gain = gain_ref[...].astype(F32)

    def finish(b, carry):
        here = pl.ds(pl.multiple_of(b * SPAN, SPAN), SPAN)
        mix = local_s[here, :]
        for d in range(2):
            start = product(entry[d], *spread_pair(prefix_s[d, b, :width, :]))
            start = start + prefix_s[d, b, width:, :]
            mix = mix + product(readout_s[d, here, :], *spread_pair(start), dims=NT)
        mean = product(mix, square, None) * (1.0 / width)
        mix = mix - mean
        spread_of = product(mix * mix, square, None) * (1.0 / width)
        mixed = mix * lax.rsqrt(spread_of + GN_EPS) * gain
        mixed_s[here, :] = mixed.astype(BF16)
        return carry

    lax.fori_loop(0, blocks, finish, 0)

    sibling = (sp, z * 2 + 1 - core)

    def sib_copy(c):
        return pltpu.make_async_remote_copy(
            src_ref=part_s.at[c, pl.ds(pl.multiple_of((1 - core) * rows, rows), rows), :],
            dst_ref=sib_s.at[c],
            send_sem=sib_send.at[c],
            recv_sem=sib_recv.at[c],
            device_id=sibling,
            device_id_type=MESH,
        )

    def z_copy(c):
        return pltpu.make_async_remote_copy(
            src_ref=summed_s.at[c],
            dst_ref=recv_s.at[z],
            send_sem=z_send.at[c],
            recv_sem=z_recv.at[z],
            device_id=(sp, c * 2 + core),
            device_id_type=MESH,
        )

    def chip_at(i):
        return lax.rem(z + 1 + i, n_z)

    def pass_on(i):
        c = chip_at(i)
        sib_copy(c).wait_recv()
        mine = part_s[c, pl.ds(pl.multiple_of(core * rows, rows), rows), :].astype(F32)
        mine = mine + sib_s[c].astype(F32)
        summed_s[c] = mine.astype(BF16)

        @pl.when(c != z)
        def _():
            z_copy(c).start()

    def project(i, carry):
        c = chip_at(i)
        there = pl.ds(pl.multiple_of(c * (2 * rows), 2 * rows), 2 * rows)
        part_s[c] = mul(mixed_s[there, :], w_ref[...]).astype(BF16)
        sib_copy(c).start()

        @pl.when(i > 0)
        def _():
            pass_on(i - 1)

        return carry

    lax.fori_loop(0, n_z, project, 0)
    pass_on(n_z - 1)
    out_ref[...] = summed_s[z].astype(F32)
    for d in range(1, n_z):
        source = lax.rem(z + d, n_z)
        pltpu.make_async_remote_copy(
            src_ref=summed_s.at[source],
            dst_ref=recv_s.at[source],
            send_sem=z_send.at[source],
            recv_sem=z_recv.at[source],
            device_id=(sp, source * 2 + core),
            device_id_type=MESH,
        ).wait_recv()
        out_ref[...] += recv_s[source].astype(F32)
        z_copy(source).wait_send()
    for c in range(n_z):
        sib_copy(c).wait_send()


def mixer(n_sp, n_tp, receptance, keys, values, erase, decay, spike, gain, weight):
    tokens, wide = keys.shape
    heads = spike.shape[1]
    width = wide // heads
    blocks = tokens // SPAN
    rows = tokens // n_tp
    n_z = n_tp // 2
    model = weight.shape[1]
    vm = pltpu.VMEM
    dma = pltpu.SemaphoreType.DMA
    return pl.pallas_call(
        functools.partial(mixer_kernel, (n_sp, n_tp, heads)),
        out_shape=jax.ShapeDtypeStruct((rows, model), F32),
        in_specs=[pl.BlockSpec(memory_space=vm)] * 8,
        out_specs=pl.BlockSpec(memory_space=vm),
        scratch_shapes=[
            vm((tokens, wide), F32),
            vm((2, tokens, wide), F32),
            vm((2, blocks, 2 * width, wide), F32),
            vm((2, blocks, 2 * width, wide), F32),
            vm((2, 2 * width, wide), BF16),
            vm((n_sp, 2 * width, wide), BF16),
            vm((tokens, wide), BF16),
            vm((n_z, 2 * rows, model), BF16),
            vm((n_z, rows, model), BF16),
            vm((n_z, rows, model), BF16),
            vm((n_z, rows, model), BF16),
            dma((n_sp,)),
            dma((n_sp,)),
            dma((n_z,)),
            dma((n_z,)),
            dma((n_z,)),
            dma((n_z,)),
        ],
        compiler_params=pltpu.CompilerParams(
            collective_id=0, has_side_effects=True, vmem_limit_bytes=56 * 1024 * 1024
        ),
        cost_estimate=pl.CostEstimate(flops=10**10, bytes_accessed=10**7, transcendentals=0),
    )(receptance, keys, values, erase, decay, spike, gain.reshape(1, wide), weight)


highest = lax.Precision.HIGHEST


def body(
    layer_input,
    receptance,
    keys,
    values,
    erase_preact,
    decay_preact,
    decay_spike,
    head_norm_gain,
    output_weight,
    expert_norm_gain,
    routes,
    routing_weight,
    expert_gate_weight,
    expert_up_weight,
    expert_down_weight,
    shared_gate_weight,
    shared_up_weight,
    shared_down_weight,
):
    row_count = layer_input.shape[0]
    model_width = layer_input.shape[1]
    projected = mixer(
        lax.axis_size("sp"), lax.axis_size("tp"), receptance, keys, values, erase_preact,
        decay_preact, decay_spike, head_norm_gain, output_weight,
    )
    residual = layer_input.astype(jnp.float32) + projected
    normed = residual * lax.rsqrt(jnp.mean(residual * residual, axis=-1, keepdims=True) + RMS_EPS)
    normed = (normed * expert_norm_gain.astype(jnp.float32)).astype(jnp.bfloat16)
    everyone = lax.all_gather(normed, "tp", axis=0, tiled=True)
    top_count = routes.shape[1]
    expert_local = expert_gate_weight.shape[0]
    sp_count = lax.axis_size("sp")
    expert_total = expert_local * sp_count
    capacity = max(2, (3 * row_count * top_count + 2 * expert_total - 1) // (2 * expert_total))
    slot_total = sp_count * capacity * expert_local
    entries = routes.reshape(-1)
    entry_count = entries.shape[0]
    expert_hot = (entries[:, None] == lax.broadcasted_iota(jnp.int32, (1, expert_total), 1)).astype(
        jnp.int32
    )
    rank_in = jnp.sum((jnp.cumsum(expert_hot, axis=0) - 1) * expert_hot, axis=1)
    slot_of = entries * capacity + rank_in
    slot_hot = (slot_of[:, None] == lax.broadcasted_iota(jnp.int32, (1, slot_total), 1)).astype(
        jnp.float32
    )
    owner_hot = (
        lax.broadcasted_iota(jnp.int32, (entry_count, 1), 0) // top_count
        == lax.broadcasted_iota(jnp.int32, (1, row_count), 1)
    ).astype(jnp.float32)
    placing = jnp.dot(slot_hot.T, owner_hot, precision=highest)
    weighting = jnp.dot(owner_hot.T, slot_hot * routing_weight.reshape(-1, 1), precision=highest)
    outgoing = jnp.dot(placing.astype(jnp.bfloat16), normed, preferred_element_type=jnp.float32)
    outgoing = outgoing.astype(jnp.bfloat16).reshape(sp_count, expert_local, capacity, model_width)
    arrived = lax.all_to_all(outgoing, "sp", split_axis=0, concat_axis=0, tiled=True)

    def gathered(rows):
        return lax.all_gather(rows, "tp", axis=0, tiled=True)

    def hidden_layer(rows, gate, up, down):
        gate_value = jnp.dot(rows, gate, preferred_element_type=jnp.float32)
        up_value = jnp.dot(rows, up, preferred_element_type=jnp.float32)
        hidden = (jax.nn.silu(gate_value) * up_value).astype(jnp.bfloat16)
        partial_rows = jnp.dot(hidden, down, preferred_element_type=jnp.float32)
        return lax.psum_scatter(
            partial_rows.astype(jnp.bfloat16), "tp", scatter_dimension=0, tiled=True
        )

    shared = hidden_layer(everyone, shared_gate_weight, shared_up_weight, shared_down_weight)
    routed_rows = []
    for j in range(expert_local):
        rows = gathered(arrived[:, j].reshape(sp_count * capacity, model_width))
        out = hidden_layer(
            rows, expert_gate_weight[j], expert_up_weight[j], expert_down_weight[j]
        )
        routed_rows.append(out.reshape(sp_count, 1, capacity, model_width))
    routed_rows = jnp.concatenate(routed_rows, axis=1)
    returned = lax.all_to_all(routed_rows, "sp", split_axis=0, concat_axis=0, tiled=True)
    routed = jnp.dot(
        weighting, returned.reshape(slot_total, model_width).astype(jnp.float32), precision=highest
    )
    return (residual + shared.astype(jnp.float32) + routed).astype(jnp.bfloat16)


def solution(mesh):
    return jax.shard_map(
        body,
        mesh=mesh,
        in_specs=(
            P(("sp", "tp"), None),
            P("sp", "tp"),
            P("sp", "tp"),
            P("sp", "tp"),
            P("sp", "tp"),
            P("sp", "tp"),
            P("sp", "tp"),
            P("tp"),
            P("tp", None),
            P(),
            P(("sp", "tp"), None),
            P(("sp", "tp"), None),
            P("sp", None, "tp"),
            P("sp", None, "tp"),
            P("sp", "tp", None),
            P(None, "tp"),
            P(None, "tp"),
            P("tp", None),
        ),
        out_specs=P(("sp", "tp"), None),
        check_vma=False,
    )
```

```python
import functools
import math
import jax
import jax.numpy as jnp
from jax import lax
from jax.experimental import pallas as pl
from jax.experimental.pallas import tpu as pltpu
from jax.sharding import PartitionSpec as P

SPAN = 64
VMEM_LIMIT = 67043328
GN_EPS = 0.00064
RMS_EPS = 1e-06
F32, BF16 = jnp.float32, jnp.bfloat16
MESH = pl.DeviceIdType.MESH
NN = (((1,), (0,)), ((), ()))
NT = (((1,), (1,)), ((), ()))
TN = (((0,), (0,)), ((), ()))


def mul(left, right, dims=NN):
    return lax.dot_general(left, right, dims, preferred_element_type=F32)


def halves(x):
    high = x.astype(BF16)
    return high, (x - high.astype(F32)).astype(BF16)


def product(left, right_high, right_low, dims=NN):
    rows = left.shape[0]
    high, low = halves(left)
    both = mul(jnp.concatenate([high, low], axis=0), right_high, dims)
    out = both[:rows] + both[rows:]
    if right_low is not None:
        out = out + mul(high, right_low, dims)
    return out


def route_table(routes, weights, experts, capacity, core):
    rows, top = routes.shape
    lanes = lax.broadcasted_iota(jnp.int32, (rows, experts), 1)
    hot = jnp.zeros((rows, experts), F32)
    weight = jnp.zeros((rows, experts), F32)
    for j in range(top):
        chosen = routes[:, j : j + 1] == lanes
        hot = hot + chosen.astype(F32)
        weight = weight + jnp.where(chosen, weights[:, j : j + 1], 0.0)
    row = lax.broadcasted_iota(jnp.int32, (rows, rows), 0)
    col = lax.broadcasted_iota(jnp.int32, (rows, rows), 1)
    rank = mul((row > col).astype(F32).astype(BF16), hot.astype(BF16))
    place = (rank + 1.0 + (core * capacity).astype(F32)) * hot
    own = lax.broadcasted_iota(jnp.int32, (rows, 2 * rows), 0) + core * rows
    shifted = (own == lax.broadcasted_iota(jnp.int32, (rows, 2 * rows), 1)).astype(F32).astype(BF16)
    part_1 = weight.astype(BF16)
    rest = weight - part_1.astype(F32)
    part_2 = rest.astype(BF16)
    part_3 = (rest - part_2.astype(F32)).astype(BF16)
    placed = mul(place.astype(BF16), shifted, TN)
    weighed = mul(part_1, shifted, TN) + mul(part_2, shifted, TN) + mul(part_3, shifted, TN)
    return jnp.concatenate([placed, weighed], axis=0)


def mixer_kernel(
    geometry,
    r_ref, k_ref, v_ref, e_ref, dp_ref, spike_ref, gain_ref, w_ref, routes_ref, rw_ref,
    out_ref, meta_ref,
    local_s, readout_s, maps_s, prefix_s, send_maps, recv_maps,
    mixed_s, part_s, sib_s, summed_s, recv_s,
    meta_s, meta_send, meta_recv, map_send, map_recv, sib_send, sib_recv, z_send, z_recv,
):
    n_sp, n_tp, heads, capacity = geometry
    n_z = n_tp // 2
    tokens, wide = k_ref.shape
    width = wide // heads
    blocks = tokens // SPAN
    rows = tokens // n_tp
    sp, tp = lax.axis_index("sp"), lax.axis_index("tp")
    z, core = tp // 2, lax.rem(tp, 2)

    barrier = pltpu.get_barrier_semaphore()
    for d in range(1, n_sp):
        pl.semaphore_signal(barrier, inc=1, device_id=(lax.rem(sp + d, n_sp), tp), device_id_type=MESH)
    for d in range(1, n_tp):
        pl.semaphore_signal(barrier, inc=1, device_id=(sp, lax.rem(tp + d, n_tp)), device_id_type=MESH)

    def head_mask(shape, dtype):
        first = lax.broadcasted_iota(jnp.int32, shape, 0) // width
        second = lax.broadcasted_iota(jnp.int32, shape, 1) // width
        return (first == second).astype(F32).astype(dtype)

    square = head_mask((wide, wide), BF16)

    def spread(x):
        return jnp.concatenate([x] * heads, axis=0) * square

    def spread_pair(x):
        high, low = halves(x)
        return spread(high), spread(low)

    def gather_heads(x):
        total = x[:width]
        for h in range(1, heads):
            total = total + x[h * width : (h + 1) * width]
        return total

    def lane_of(shape):
        return lax.broadcasted_iota(jnp.int32, shape, 1)

    row_t = lax.broadcasted_iota(jnp.int32, (SPAN, wide), 0)
    col_s = lax.rem(lane_of((SPAN, wide)), SPAN)
    below = row_t > col_s
    above = row_t < col_s
    same = row_t == col_s
    tri = (
        lax.broadcasted_iota(jnp.int32, (SPAN, SPAN), 0)
        >= lax.broadcasted_iota(jnp.int32, (SPAN, SPAN), 1)
    ).astype(F32).astype(BF16)
    tri3 = jnp.concatenate([tri, tri, tri], axis=1)
    eye = same.astype(F32)

    def each_block(b, carry):
        here = pl.ds(pl.multiple_of(b * SPAN, SPAN), SPAN)
        keys = k_ref[here, :].astype(F32)
        square_high, square_low = halves(keys * keys)
        norm = mul(jnp.concatenate([square_high, square_low], axis=0), square)
        norm = norm[:SPAN] + norm[SPAN:]
        unit = keys * lax.rsqrt(norm + 1e-06)
        beta = unit * jax.nn.sigmoid(e_ref[here, :].astype(F32))
        spikes = spike_ref[here, :]
        lane_head = lane_of((SPAN, wide)) // width
        spike = jnp.zeros((SPAN, wide), F32)
        for h in range(heads):
            spike = jnp.where(lane_head == h, spikes[:, h : h + 1], spike)
        decay = -0.6065306597126334 * jax.nn.sigmoid(dp_ref[here, :].astype(F32)) + spike
        decay_1 = decay.astype(BF16)
        rest = decay - decay_1.astype(F32)
        decay_2 = rest.astype(BF16)
        decay_3 = (rest - decay_2.astype(F32)).astype(BF16)
        cumulative = mul(tri3, jnp.concatenate([decay_1, decay_2, decay_3], axis=0))
        total = cumulative[SPAN - 1 : SPAN, :]
        middle = 0.5 * total
        e1 = jnp.exp(cumulative - middle)
        e2 = jnp.exp(cumulative - decay - middle)
        e3 = jnp.exp(middle - cumulative)
        e4 = jnp.exp(middle - cumulative + decay)
        em = jnp.exp(middle)
        et = jnp.exp(total)
        reads = r_ref[here, :].astype(F32)
        values = v_ref[here, :]
        value_wide = spread(values)
        local_sum = jnp.zeros((SPAN, wide), F32)
        for d in range(2):
            strict = below if d == 0 else above
            loose = strict | same
            left_scale, before_scale, right_scale = (e1, e2, e3) if d == 0 else (e4, e3, e2)
            left = jnp.concatenate([unit * before_scale, reads * left_scale], axis=0)
            beta_right = beta * right_scale
            key_right = keys * right_scale
            keep = jnp.concatenate([strict, loose], axis=0)
            from_beta = jnp.where(keep, product(left, *spread_pair(beta_right), dims=NT), 0.0)
            from_key = jnp.where(keep, product(left, *spread_pair(key_right), dims=NT), 0.0)
            key_part = product(from_key, value_wide, None)
            corner_all = from_beta[:SPAN]
            size, inverse = 1, None
            while size < SPAN:
                joined = row_t // (2 * size) == col_s // (2 * size)
                corner = jnp.where(joined & (row_t // size != col_s // size), corner_all, 0.0)
                if size == 1:
                    inverse = eye - corner
                else:
                    pair = spread_pair(inverse)
                    step = product(corner, *pair)
                    inverse = inverse - product(inverse, *spread_pair(step))
                size *= 2
            true_left = left * em
            solved_w = product(inverse, *spread_pair(true_left[:SPAN]))
            solved_v = product(inverse, *spread_pair(-key_part[:SPAN]))
            read = from_beta[SPAN:]
            local_sum = local_sum + key_part[SPAN:] + product(read, *spread_pair(solved_v))
            readout_s[d, here, :] = true_left[SPAN:] - product(read, *spread_pair(solved_w))
            beta_high, beta_low = halves(beta_right * em)
            key_high, key_low = halves(key_right * em)
            w_high, w_low = halves(solved_w)
            v_high, v_low = halves(solved_v)
            beta_three = [beta_high, beta_low, beta_high]
            move = mul(
                jnp.concatenate([w_high, w_high, w_low], axis=0),
                jnp.concatenate(beta_three, axis=0),
                TN,
            )
            put = mul(
                jnp.concatenate([v_high, v_high, v_low, values, values], axis=0),
                jnp.concatenate(beta_three + [key_high, key_low], axis=0),
                TN,
            )
            on_head = lax.broadcasted_iota(jnp.int32, (width, wide), 0) == lax.rem(
                lane_of((width, wide)), width
            )
            wide_mask = square.astype(F32)
            move = gather_heads(move * wide_mask)
            maps_s[d, b, :width, :] = jnp.where(on_head, et, 0.0) - move
            maps_s[d, b, width:, :] = gather_heads(put * wide_mask)
        local_s[here, :] = local_sum
        return carry

    lax.fori_loop(0, blocks, each_block, 0)

    first = (
        lax.broadcasted_iota(jnp.int32, (2 * width, wide), 0)
        == lax.rem(lane_of((2 * width, wide)), width)
    ).astype(F32)
    no_rows = jnp.zeros((width, wide), F32)

    def compose(i, carry):
        new = []
        for d in range(2):
            b = i if d == 0 else blocks - 1 - i
            prefix_s[d, b] = carry[d]
            moved = product(carry[d], *spread_pair(maps_s[d, b, :width, :]))
            new.append(moved + jnp.concatenate([no_rows, maps_s[d, b, width:, :]], axis=0))
        return tuple(new)

    whole = lax.fori_loop(0, blocks, compose, (first, first))
    for d in range(2):
        send_maps[d] = whole[d].astype(BF16)
    pl.semaphore_wait(barrier, n_sp - 1 + n_tp - 1)

    experts = meta_ref.shape[1] // 2
    meta_s[tp] = route_table(routes_ref[...], rw_ref[...], experts, capacity, core)

    def meta_copy(d):
        return pltpu.make_async_remote_copy(
            src_ref=meta_s.at[tp],
            dst_ref=meta_s.at[tp],
            send_sem=meta_send.at[d],
            recv_sem=meta_recv.at[tp],
            device_id=(sp, lax.rem(tp + d, n_tp)),
            device_id_type=MESH,
        )

    for d in range(1, n_tp):
        meta_copy(d).start()

    copies = []
    for d in range(1, n_sp):
        target = lax.rem(sp + d, n_sp)
        copy = pltpu.make_async_remote_copy(
            src_ref=send_maps.at[(target < sp).astype(jnp.int32)],
            dst_ref=recv_maps.at[sp],
            send_sem=map_send.at[d],
            recv_sem=map_recv.at[sp],
            device_id=(target, tp),
            device_id_type=MESH,
        )
        copy.start()
        copies.append(copy)
    for d in range(1, n_sp):
        source = lax.rem(sp + d, n_sp)
        pltpu.make_async_remote_copy(
            src_ref=send_maps.at[0],
            dst_ref=recv_maps.at[source],
            send_sem=map_send.at[d],
            recv_sem=map_recv.at[source],
            device_id=(source, tp),
            device_id_type=MESH,
        ).wait_recv()
    for copy in copies:
        copy.wait_send()
    recv_maps[sp] = jnp.zeros((2 * width, wide), BF16)

    def enter(i, carry):
        new = []
        for d in range(2):
            k = i if d == 0 else n_sp - 1 - i
            reached = (k < sp) if d == 0 else (k > sp)
            part = recv_maps[k]
            moved = product(carry[d], spread(part[:width]), None) + part[width:].astype(F32)
            new.append(jnp.where(reached, moved, carry[d]))
        return tuple(new)

    entry = lax.fori_loop(0, n_sp, enter, (no_rows, no_rows))

    gain = gain_ref[...].astype(F32)

    def finish(b, carry):
        here = pl.ds(pl.multiple_of(b * SPAN, SPAN), SPAN)
        mix = local_s[here, :]
        for d in range(2):
            start = product(entry[d], *spread_pair(prefix_s[d, b, :width, :]))
            start = start + prefix_s[d, b, width:, :]
            mix = mix + product(readout_s[d, here, :], *spread_pair(start), dims=NT)
        mean = product(mix, square, None) * (1.0 / width)
        mix = mix - mean
        spread_of = product(mix * mix, square, None) * (1.0 / width)
        mixed = mix * lax.rsqrt(spread_of + GN_EPS) * gain
        mixed_s[here, :] = mixed.astype(BF16)
        return carry

    lax.fori_loop(0, blocks, finish, 0)

    sibling = (sp, z * 2 + 1 - core)

    def sib_copy(c):
        return pltpu.make_async_remote_copy(
            src_ref=part_s.at[c, pl.ds(pl.multiple_of((1 - core) * rows, rows), rows), :],
            dst_ref=sib_s.at[c],
            send_sem=sib_send.at[c],
            recv_sem=sib_recv.at[c],
            device_id=sibling,
            device_id_type=MESH,
        )

    def z_copy(c):
        return pltpu.make_async_remote_copy(
            src_ref=summed_s.at[c],
            dst_ref=recv_s.at[z],
            send_sem=z_send.at[c],
            recv_sem=z_recv.at[z],
            device_id=(sp, c * 2 + core),
            device_id_type=MESH,
        )

    def chip_at(i):
        return lax.rem(z + 1 + i, n_z)

    def pass_on(i):
        c = chip_at(i)
        sib_copy(c).wait_recv()
        mine = part_s[c, pl.ds(pl.multiple_of(core * rows, rows), rows), :].astype(F32)
        mine = mine + sib_s[c].astype(F32)
        summed_s[c] = mine.astype(BF16)

        @pl.when(c != z)
        def _():
            z_copy(c).start()

    def project(i, carry):
        c = chip_at(i)
        there = pl.ds(pl.multiple_of(c * (2 * rows), 2 * rows), 2 * rows)
        part_s[c] = mul(mixed_s[there, :], w_ref[...]).astype(BF16)
        sib_copy(c).start()

        @pl.when(i > 0)
        def _():
            pass_on(i - 1)

        return carry

    lax.fori_loop(0, n_z, project, 0)
    pass_on(n_z - 1)
    out_ref[...] = summed_s[z].astype(F32)
    for d in range(1, n_z):
        source = lax.rem(z + d, n_z)
        pltpu.make_async_remote_copy(
            src_ref=summed_s.at[source],
            dst_ref=recv_s.at[source],
            send_sem=z_send.at[source],
            recv_sem=z_recv.at[source],
            device_id=(sp, source * 2 + core),
            device_id_type=MESH,
        ).wait_recv()
        out_ref[...] += recv_s[source].astype(F32)
        z_copy(source).wait_send()
    for c in range(n_z):
        sib_copy(c).wait_send()
    for d in range(1, n_tp):
        source = lax.rem(tp + d, n_tp)
        pltpu.make_async_remote_copy(
            src_ref=meta_s.at[tp],
            dst_ref=meta_s.at[source],
            send_sem=meta_send.at[d],
            recv_sem=meta_recv.at[source],
            device_id=(sp, source),
            device_id_type=MESH,
        ).wait_recv()
        meta_copy(d).wait_send()
    meta_ref[...] = meta_s[...]


def mixer(n_sp, n_tp, receptance, keys, values, erase, decay, spike, gain, weight, routes, routing, experts, capacity):
    tokens, wide = keys.shape
    heads = spike.shape[1]
    width = wide // heads
    blocks = tokens // SPAN
    rows = tokens // n_tp
    n_z = n_tp // 2
    model = weight.shape[1]
    vm = pltpu.VMEM
    dma = pltpu.SemaphoreType.DMA
    return pl.pallas_call(
        functools.partial(mixer_kernel, (n_sp, n_tp, heads, capacity)),
        out_shape=[
            jax.ShapeDtypeStruct((rows, model), F32),
            jax.ShapeDtypeStruct((n_tp, 2 * experts, 2 * rows), F32),
        ],
        in_specs=[pl.BlockSpec(memory_space=vm)] * 10,
        out_specs=[pl.BlockSpec(memory_space=vm)] * 2,
        scratch_shapes=[
            vm((tokens, wide), F32),
            vm((2, tokens, wide), F32),
            vm((2, blocks, 2 * width, wide), F32),
            vm((2, blocks, 2 * width, wide), F32),
            vm((2, 2 * width, wide), BF16),
            vm((n_sp, 2 * width, wide), BF16),
            vm((tokens, wide), BF16),
            vm((n_z, 2 * rows, model), BF16),
            vm((n_z, rows, model), BF16),
            vm((n_z, rows, model), BF16),
            vm((n_z, rows, model), BF16),
            vm((n_tp, 2 * experts, 2 * rows), F32),
            dma((n_tp,)),
            dma((n_tp,)),
            dma((n_sp,)),
            dma((n_sp,)),
            dma((n_z,)),
            dma((n_z,)),
            dma((n_z,)),
            dma((n_z,)),
        ],
        compiler_params=pltpu.CompilerParams(
            collective_id=0, has_side_effects=True, vmem_limit_bytes=56 * 1024 * 1024
        ),
        cost_estimate=pl.CostEstimate(flops=10**10, bytes_accessed=10**7, transcendentals=0),
    )(receptance, keys, values, erase, decay, spike, gain.reshape(1, wide), weight, routes, routing)


def expert_kernel(
    geometry,
    input_ref, projected_ref, gain_ref, meta_ref, gate_hbm, up_hbm, down_hbm,
    shared_gate_hbm, shared_up_hbm, shared_down_hbm, out_ref,
    gate, up, down, shared_gate, shared_up, shared_down,
    residual, table, own, xg, sel_out, sel_in, y_buf, y_sib, sh_buf, sh_sib,
    q_out, q_in, t_out, t_in, fin, fin_sib,
    w_sem, own_sem, z_send, z_recv, xr_send, xr_recv, sel_send, sel_recv, sr_send, sr_recv,
    y_send, y_recv, sh_send, sh_recv, q_send, q_recv, t_send, t_recv, fin_sem,
):
    n_sp, n_tp, capacity = geometry
    n_z = n_tp // 2
    rows, model = input_ref.shape
    half = model // 2
    pair = 2 * rows
    slots = 2 * capacity
    local = gate_hbm.shape[0]
    experts = meta_ref.shape[1] // 2
    hidden = gate_hbm.shape[2]
    sp, tp = lax.axis_index("sp"), lax.axis_index("tp")
    z, core = tp // 2, lax.rem(tp, 2)
    other = 1 - core
    sibling = (sp, z * 2 + other)

    barrier = pltpu.get_barrier_semaphore()
    for d in range(1, n_sp):
        pl.semaphore_signal(barrier, inc=1, device_id=(lax.rem(sp + d, n_sp), tp), device_id_type=MESH)
    for d in range(1, n_z):
        pl.semaphore_signal(
            barrier, inc=1, device_id=(sp, lax.rem(z + d, n_z) * 2 + core), device_id_type=MESH
        )
    pl.semaphore_signal(barrier, inc=1, device_id=sibling, device_id_type=MESH)

    loads = [
        pltpu.make_async_copy(source, target, w_sem.at[i])
        for i, (source, target) in enumerate(
            [
                (gate_hbm, gate), (up_hbm, up), (down_hbm, down), (shared_gate_hbm, shared_gate),
                (shared_up_hbm, shared_up), (shared_down_hbm, shared_down),
            ]
        )
    ]
    for load in loads:
        load.start()

    def remote(source, target, send, recv, device):
        return pltpu.make_async_remote_copy(
            src_ref=source, dst_ref=target, send_sem=send, recv_sem=recv,
            device_id=device, device_id_type=MESH,
        )

    def rows_at(c):
        return pl.ds(pl.multiple_of(c * rows, rows), rows)

    total = input_ref[...].astype(F32) + projected_ref[...]
    residual[...] = total
    normed = total * lax.rsqrt(jnp.mean(total * total, axis=-1, keepdims=True) + RMS_EPS)
    normed = (normed * gain_ref[...].astype(F32)).astype(BF16)
    for h in range(2):
        own[h] = normed[:, h * half : (h + 1) * half]
        xg[z, h, rows_at(core), :] = normed[:, h * half : (h + 1) * half]
    for c in range(n_z):
        table[c] = meta_ref[2 * c] + meta_ref[2 * c + 1]
    pl.semaphore_wait(barrier, n_sp - 1 + n_z)

    own_copy = remote(own, xg.at[z, :, rows_at(core), :], own_sem.at[0], own_sem.at[1], sibling)
    own_copy.start()
    own_copy.wait_recv()

    def z_copy(c, target):
        return remote(xg.at[c, core], xg.at[c, core], z_send.at[target], z_recv.at[c], (sp, target * 2 + core))

    for d in range(1, n_z):
        z_copy(z, lax.rem(z + n_z - d, n_z)).start()

    def relay_x(c):
        return remote(xg.at[c, core], xg.at[c, core], xr_send.at[c], xr_recv.at[c], sibling)

    def relay_x_in(c):
        return remote(xg.at[c, other], xg.at[c, other], xr_send.at[c], xr_recv.at[c], sibling)

    def sel_copy(c, g):
        return remote(
            sel_out.at[c, g], sel_in.at[c, core, :, sp], sel_send.at[c, g], sel_recv.at[c, sp],
            (g, tp),
        )

    def sel_arrival(c, g):
        return remote(
            sel_out.at[c, g], sel_in.at[c, core, :, g], sel_send.at[c, g], sel_recv.at[c, g], (g, tp)
        )

    def relay_sel(c, g):
        there = sel_in.at[c, core, :, g]
        return remote(there, there, sr_send.at[c, g], sr_recv.at[c, g], sibling)

    def relay_sel_in(c, g):
        there = sel_in.at[c, other, :, g]
        return remote(there, there, sr_send.at[c, g], sr_recv.at[c, g], sibling)

    slot_ids = (lax.broadcasted_iota(jnp.int32, (slots, pair), 0) + 1).astype(F32)

    def picks(c, g):
        return [(slot_ids == table[c, pl.ds(g * local + j, 1), :]).astype(F32) for j in range(local)]

    def select(c, g, h):
        chosen = jnp.concatenate(picks(c, g), axis=0).astype(BF16)
        return mul(chosen, xg[c, h]).astype(BF16).reshape(local, slots, half)

    def send_rows(c):
        for d in range(1, n_sp):
            g = lax.rem(sp + d, n_sp)
            sel_out[c, g] = select(c, g, core)
            sel_copy(c, g).start()

    send_rows(z)
    for load in loads:
        load.wait()

    def feed(x, first, second):
        gate_value = mul(x[0], first[:half, :]) + mul(x[1], first[half:, :])
        up_value = mul(x[0], second[:half, :]) + mul(x[1], second[half:, :])
        return (jax.nn.silu(gate_value) * up_value).astype(BF16)

    def y_copy(c):
        return remote(y_buf.at[c, other], y_sib.at[c], y_send.at[c], y_recv.at[c], sibling)

    def sh_copy(c):
        return remote(sh_buf.at[c, other], sh_sib.at[c], sh_send.at[c], sh_recv.at[c], sibling)

    def q_copy(c, g):
        return remote(q_out.at[c, :, g], q_in.at[c, :, sp], q_send.at[c, g], q_recv.at[c, sp], (g, tp))

    def q_arrival(c, g):
        return remote(q_out.at[c, :, g], q_in.at[c, :, g], q_send.at[c, g], q_recv.at[c, g], (g, tp))

    def t_copy(c):
        return remote(t_out.at[c], t_in.at[z], t_send.at[c], t_recv.at[z], (sp, c * 2 + core))

    def t_arrival(c):
        return remote(t_out.at[c], t_in.at[c], t_send.at[c], t_recv.at[c], (sp, c * 2 + core))

    def combine(c):
        for d in range(1, n_sp):
            q_arrival(c, lax.rem(sp + d, n_sp)).wait_recv()
        result = sh_buf[c, core].astype(F32) + sh_sib[c].astype(F32)
        for j in range(local):
            weighted = []
            for g in range(n_sp):
                hot = slot_ids == table[c, g * local + j : g * local + j + 1, :]
                weight = table[c, experts + g * local + j : experts + g * local + j + 1, :]
                weighted.append(jnp.where(hot, weight, 0.0))
            high, low = halves(jnp.concatenate(weighted, axis=0))
            values = q_in[c, j].reshape(n_sp * slots, half)
            result = result + mul(high, values, TN) + mul(low, values, TN)
        return result

    def pass_on(c):
        t_out[c] = combine(c).astype(BF16)
        t_copy(c).start()

    def step(k, carry):
        c = lax.rem(z + k, n_z)

        @pl.when(k < n_z - 1)
        def _():
            later = lax.rem(z + k + 1, n_z)
            z_copy(later, z).wait_recv()
            relay_x(later).start()
            send_rows(later)

        for d in range(1, n_sp):
            g = lax.rem(sp + n_sp - d, n_sp)
            sel_arrival(c, g).wait_recv()
            relay_sel(c, g).start()

        @pl.when(k > 0)
        def _():
            relay_x_in(c).wait_recv()

        for h in range(2):
            sel_in[c, h, :, sp] = select(c, sp, h)
        hidden_rows = feed([xg[c, 0], xg[c, 1]], shared_gate, shared_up)
        for h in range(2):
            sh_buf[c, h] = mul(hidden_rows, shared_down[:, h * half : (h + 1) * half]).astype(BF16)
        sh_copy(c).start()
        for d in range(1, n_sp):
            relay_sel_in(c, lax.rem(sp + n_sp - d, n_sp)).wait_recv()
        for j in range(local):
            x = [sel_in[c, h, j].reshape(n_sp * slots, half) for h in range(2)]
            hidden_rows = feed(x, gate.at[j], up.at[j])
            for h in range(2):
                y = mul(hidden_rows, down[j, :, h * half : (h + 1) * half]).astype(BF16)
                y_buf[c, h, j] = y.reshape(n_sp, slots, half)
        y_copy(c).start()

        @pl.when(k > 1)
        def _():
            pass_on(lax.rem(z + k - 1, n_z))

        y_copy(c).wait_recv()
        sh_copy(c).wait_recv()
        q_out[c] = (y_buf[c, core].astype(F32) + y_sib[c].astype(F32)).astype(BF16)
        q_in[c, :, sp] = q_out[c, :, sp]
        for d in range(1, n_sp):
            q_copy(c, lax.rem(sp + d, n_sp)).start()
        return carry

    lax.fori_loop(0, n_z, step, 0)
    pass_on(lax.rem(z + n_z - 1, n_z))
    fin[...] = combine(z)
    for d in range(1, n_z):
        c = lax.rem(z + d, n_z)
        t_arrival(c).wait_recv()
        fin[...] += t_in[c].astype(F32)
    fin_copy = remote(fin.at[rows_at(other), :], fin_sib, fin_sem.at[0], fin_sem.at[1], sibling)
    fin_copy.start()

    def columns(c):
        return pl.ds(pl.multiple_of(c * half, half), half)

    mine = residual[:, columns(core)] + fin[rows_at(core), :]
    out_ref[:, columns(core)] = mine.astype(out_ref.dtype)
    fin_copy.wait_recv()
    theirs = residual[:, columns(other)] + fin_sib[...]
    out_ref[:, columns(other)] = theirs.astype(out_ref.dtype)
    fin_copy.wait_send()
    own_copy.wait_send()
    for c in range(n_z):
        y_copy(c).wait_send()
        sh_copy(c).wait_send()
        for d in range(1, n_sp):
            g = lax.rem(sp + d, n_sp)
            sel_copy(c, g).wait_send()
            relay_sel(c, g).wait_send()
            q_copy(c, g).wait_send()
    for d in range(1, n_z):
        c = lax.rem(z + d, n_z)
        z_copy(z, c).wait_send()
        relay_x(c).wait_send()
        t_copy(c).wait_send()


def expert_shapes(n_sp, n_tp, rows, model, local, hidden, experts, capacity):
    n_z, half, pair, slots = n_tp // 2, model // 2, 2 * rows, 2 * capacity
    return [
        ((local, model, hidden), BF16),
        ((local, model, hidden), BF16),
        ((local, hidden, model), BF16),
        ((model, hidden), BF16),
        ((model, hidden), BF16),
        ((hidden, model), BF16),
        ((rows, model), F32),
        ((n_z, 2 * experts, pair), F32),
        ((2, rows, half), BF16),
        ((n_z, 2, pair, half), BF16),
        ((n_z, n_sp, local, slots, half), BF16),
        ((n_z, 2, local, n_sp, slots, half), BF16),
        ((n_z, 2, local, n_sp, slots, half), BF16),
        ((n_z, local, n_sp, slots, half), BF16),
        ((n_z, 2, pair, half), BF16),
        ((n_z, pair, half), BF16),
        ((n_z, local, n_sp, slots, half), BF16),
        ((n_z, local, n_sp, slots, half), BF16),
        ((n_z, pair, half), BF16),
        ((n_z, pair, half), BF16),
        ((pair, half), F32),
        ((rows, half), F32),
    ]


def expert_layer(
    n_sp, n_tp, shapes, capacity, layer_input, projected, gain, meta, gate, up, down,
    shared_gate, shared_up, shared_down,
):
    n_z = n_tp // 2
    vm = pltpu.VMEM
    dma = pltpu.SemaphoreType.DMA
    inside, outside = pl.BlockSpec(memory_space=vm), pl.BlockSpec(memory_space=pl.ANY)
    one, two = dma((n_z,)), dma((n_z, n_sp))
    return pl.pallas_call(
        functools.partial(expert_kernel, (n_sp, n_tp, capacity)),
        out_shape=jax.ShapeDtypeStruct(layer_input.shape, BF16),
        in_specs=[inside] * 4 + [outside] * 6,
        out_specs=inside,
        scratch_shapes=[vm(shape, dtype) for shape, dtype in shapes]
        + [dma((6,)), dma((2,)), one, one, one, one, two, two, two, two]
        + [one, one, one, one, two, two, one, one, dma((2,))],
        compiler_params=pltpu.CompilerParams(
            collective_id=1, has_side_effects=True, vmem_limit_bytes=VMEM_LIMIT
        ),
        cost_estimate=pl.CostEstimate(flops=10**10, bytes_accessed=10**7, transcendentals=0),
    )(
        layer_input, projected, gain.reshape(1, -1), meta, gate, up, down,
        shared_gate, shared_up, shared_down,
    )


highest = lax.Precision.HIGHEST


def body(
    layer_input,
    receptance,
    keys,
    values,
    erase_preact,
    decay_preact,
    decay_spike,
    head_norm_gain,
    output_weight,
    expert_norm_gain,
    routes,
    routing_weight,
    expert_gate_weight,
    expert_up_weight,
    expert_down_weight,
    shared_gate_weight,
    shared_up_weight,
    shared_down_weight,
):
    row_count, model_width = layer_input.shape
    top_count = routes.shape[1]
    expert_local = expert_gate_weight.shape[0]
    sp_count, tp_count = lax.axis_size("sp"), lax.axis_size("tp")
    expert_total = expert_local * sp_count
    capacity = max(2, (3 * row_count * top_count + 2 * expert_total - 1) // (2 * expert_total))
    slot_total = sp_count * capacity * expert_local
    projected, meta = mixer(
        sp_count, tp_count, receptance, keys, values, erase_preact, decay_preact, decay_spike,
        head_norm_gain, output_weight, routes, routing_weight, expert_total, capacity,
    )
    shapes = expert_shapes(
        sp_count, tp_count, row_count, model_width, expert_local, expert_gate_weight.shape[2],
        expert_total, capacity,
    )
    used = sum(math.prod(shape) * jnp.dtype(dtype).itemsize for shape, dtype in shapes)
    if used < VMEM_LIMIT * 7 // 8 and (2 * capacity) % 16 == 0:
        return expert_layer(
            sp_count, tp_count, shapes, capacity, layer_input, projected, expert_norm_gain, meta,
            expert_gate_weight, expert_up_weight, expert_down_weight,
            shared_gate_weight, shared_up_weight, shared_down_weight,
        )
    residual = layer_input.astype(jnp.float32) + projected
    normed = residual * lax.rsqrt(jnp.mean(residual * residual, axis=-1, keepdims=True) + RMS_EPS)
    normed = (normed * expert_norm_gain.astype(jnp.float32)).astype(jnp.bfloat16)
    everyone = lax.all_gather(normed, "tp", axis=0, tiled=True)
    entries = routes.reshape(-1)
    entry_count = entries.shape[0]
    expert_hot = (entries[:, None] == lax.broadcasted_iota(jnp.int32, (1, expert_total), 1)).astype(
        jnp.int32
    )
    rank_in = jnp.sum((jnp.cumsum(expert_hot, axis=0) - 1) * expert_hot, axis=1)
    slot_of = entries * capacity + rank_in
    slot_hot = (slot_of[:, None] == lax.broadcasted_iota(jnp.int32, (1, slot_total), 1)).astype(
        jnp.float32
    )
    owner_hot = (
        lax.broadcasted_iota(jnp.int32, (entry_count, 1), 0) // top_count
        == lax.broadcasted_iota(jnp.int32, (1, row_count), 1)
    ).astype(jnp.float32)
    placing = jnp.dot(slot_hot.T, owner_hot, precision=highest)
    weighting = jnp.dot(owner_hot.T, slot_hot * routing_weight.reshape(-1, 1), precision=highest)
    outgoing = jnp.dot(placing.astype(jnp.bfloat16), normed, preferred_element_type=jnp.float32)
    outgoing = outgoing.astype(jnp.bfloat16).reshape(sp_count, expert_local, capacity, model_width)
    arrived = lax.all_to_all(outgoing, "sp", split_axis=0, concat_axis=0, tiled=True)

    def gathered(rows):
        return lax.all_gather(rows, "tp", axis=0, tiled=True)

    def hidden_layer(rows, gate, up, down):
        gate_value = jnp.dot(rows, gate, preferred_element_type=jnp.float32)
        up_value = jnp.dot(rows, up, preferred_element_type=jnp.float32)
        hidden = (jax.nn.silu(gate_value) * up_value).astype(jnp.bfloat16)
        partial_rows = jnp.dot(hidden, down, preferred_element_type=jnp.float32)
        return lax.psum_scatter(
            partial_rows.astype(jnp.bfloat16), "tp", scatter_dimension=0, tiled=True
        )

    shared = hidden_layer(everyone, shared_gate_weight, shared_up_weight, shared_down_weight)
    routed_rows = []
    for j in range(expert_local):
        rows = gathered(arrived[:, j].reshape(sp_count * capacity, model_width))
        out = hidden_layer(
            rows, expert_gate_weight[j], expert_up_weight[j], expert_down_weight[j]
        )
        routed_rows.append(out.reshape(sp_count, 1, capacity, model_width))
    routed_rows = jnp.concatenate(routed_rows, axis=1)
    returned = lax.all_to_all(routed_rows, "sp", split_axis=0, concat_axis=0, tiled=True)
    routed = jnp.dot(
        weighting, returned.reshape(slot_total, model_width).astype(jnp.float32), precision=highest
    )
    return (residual + shared.astype(jnp.float32) + routed).astype(jnp.bfloat16)


def solution(mesh):
    return jax.shard_map(
        body,
        mesh=mesh,
        in_specs=(
            P(("sp", "tp"), None),
            P("sp", "tp"),
            P("sp", "tp"),
            P("sp", "tp"),
            P("sp", "tp"),
            P("sp", "tp"),
            P("sp", "tp"),
            P("tp"),
            P("tp", None),
            P(),
            P(("sp", "tp"), None),
            P(("sp", "tp"), None),
            P("sp", None, "tp"),
            P("sp", None, "tp"),
            P("sp", "tp", None),
            P(None, "tp"),
            P(None, "tp"),
            P("tp", None),
        ),
        out_specs=P(("sp", "tp"), None),
        check_vma=False,
    )
```

```python
import functools
import math
import jax
import jax.numpy as jnp
from jax import lax
from jax.experimental import pallas as pl
from jax.experimental.pallas import tpu as pltpu
from jax.sharding import PartitionSpec as P

SPAN = 64
TOGETHER = 4
VMEM_LIMIT = 67043328
GN_EPS = 0.00064
RMS_EPS = 1e-06
F32, BF16 = jnp.float32, jnp.bfloat16
MESH = pl.DeviceIdType.MESH
NN = (((1,), (0,)), ((), ()))
NT = (((1,), (1,)), ((), ()))
TN = (((0,), (0,)), ((), ()))


def mul(left, right, dims=NN):
    return lax.dot_general(left, right, dims, preferred_element_type=F32)


def halves(x):
    high = x.astype(BF16)
    return high, (x - high.astype(F32)).astype(BF16)


def thirds(x):
    first = x.astype(BF16)
    rest = x - first.astype(F32)
    second = rest.astype(BF16)
    return first, second, (rest - second.astype(F32)).astype(BF16)


def product(left, right_high, right_low, dims=NN):
    rows = left.shape[0]
    high, low = halves(left)
    both = mul(jnp.concatenate([high, low], axis=0), right_high, dims)
    out = both[:rows] + both[rows:]
    if right_low is not None:
        out = out + mul(high, right_low, dims)
    return out


def route_table(routes, weights, experts, capacity, core):
    top, rows = routes.shape
    lines = lax.broadcasted_iota(jnp.int32, (experts, rows), 0)
    hot = jnp.zeros((experts, rows), F32)
    weight = jnp.zeros((experts, rows), F32)
    for j in range(top):
        chosen = routes[j : j + 1, :] == lines
        hot = hot + chosen.astype(F32)
        weight = weight + jnp.where(chosen, weights[j : j + 1, :], 0.0)
    row = lax.broadcasted_iota(jnp.int32, (rows, rows), 0)
    col = lax.broadcasted_iota(jnp.int32, (rows, rows), 1)
    rank = mul(hot.astype(BF16), (row < col).astype(F32).astype(BF16))
    place = (rank + 1.0 + (core * capacity).astype(F32)) * hot
    own = lax.broadcasted_iota(jnp.int32, (rows, 2 * rows), 0) + core * rows
    shifted = (own == lax.broadcasted_iota(jnp.int32, (rows, 2 * rows), 1)).astype(F32).astype(BF16)
    placed = mul(place.astype(BF16), shifted)
    weighed = sum(mul(part, shifted) for part in thirds(weight))
    return jnp.concatenate([placed, weighed], axis=0)


def mixer_kernel(
    geometry,
    r_ref, k_ref, v_ref, e_ref, dp_ref, spike_ref, gain_ref, w_ref, routes_ref, rw_ref,
    out_ref, meta_ref,
    spike_s, local_s, readout_s, maps_s, prefix_s, send_maps, recv_maps,
    mixed_s, part_s, sib_s, summed_s, recv_s,
    meta_s, meta_send, meta_recv, map_send, map_recv, sib_send, sib_recv, z_send, z_recv,
):
    n_sp, n_tp, heads, capacity = geometry
    n_z = n_tp // 2
    tokens, wide = k_ref.shape
    width = wide // heads
    blocks = tokens // SPAN
    rows = tokens // n_tp
    sp, tp = lax.axis_index("sp"), lax.axis_index("tp")
    z, core = tp // 2, lax.rem(tp, 2)

    barrier = pltpu.get_barrier_semaphore()
    for d in range(1, n_sp):
        pl.semaphore_signal(barrier, inc=1, device_id=(lax.rem(sp + d, n_sp), tp), device_id_type=MESH)
    for d in range(1, n_tp):
        pl.semaphore_signal(barrier, inc=1, device_id=(sp, lax.rem(tp + d, n_tp)), device_id_type=MESH)

    def head_mask(shape, dtype):
        first = lax.broadcasted_iota(jnp.int32, shape, 0) // width
        second = lax.broadcasted_iota(jnp.int32, shape, 1) // width
        return (first == second).astype(F32).astype(dtype)

    square = head_mask((wide, wide), BF16)

    def spread(x):
        return jnp.concatenate([x] * heads, axis=0) * square

    def spread_pair(x):
        high, low = halves(x)
        return spread(high), spread(low)

    def gather_heads(x):
        total = x[:width]
        for h in range(1, heads):
            total = total + x[h * width : (h + 1) * width]
        return total

    def lane_of(shape):
        return lax.broadcasted_iota(jnp.int32, shape, 1)

    row_t = lax.broadcasted_iota(jnp.int32, (SPAN, wide), 0)
    col_s = lax.rem(lane_of((SPAN, wide)), SPAN)
    below = row_t > col_s
    above = row_t < col_s
    same = row_t == col_s
    tri = (
        lax.broadcasted_iota(jnp.int32, (SPAN, SPAN), 0)
        >= lax.broadcasted_iota(jnp.int32, (SPAN, SPAN), 1)
    ).astype(F32).astype(BF16)
    tri3 = jnp.concatenate([tri, tri, tri], axis=1)
    eye = same.astype(F32)

    def product_all(lefts, rights, dims=NN):
        pairs = [spread_pair(right) for right in rights]
        return [product(left, *pair, dims=dims) for left, pair in zip(lefts, pairs)]

    def each_group(i, carry):
        chains = []
        blocks_here = []
        for b in [i * TOGETHER + n for n in range(TOGETHER)]:
            here = pl.ds(pl.multiple_of(b * SPAN, SPAN), SPAN)
            keys = k_ref[here, :].astype(F32)
            square_high, square_low = halves(keys * keys)
            norm = mul(jnp.concatenate([square_high, square_low], axis=0), square)
            norm = norm[:SPAN] + norm[SPAN:]
            unit = keys * lax.rsqrt(norm + 1e-06)
            beta = unit * jax.nn.sigmoid(e_ref[here, :].astype(F32))
            decay = -0.6065306597126334 * jax.nn.sigmoid(dp_ref[here, :].astype(F32))
            decay = decay + spike_s[here, :]
            decay_1, decay_2, decay_3 = thirds(decay)
            cumulative = mul(tri3, jnp.concatenate([decay_1, decay_2, decay_3], axis=0))
            total = cumulative[SPAN - 1 : SPAN, :]
            middle = 0.5 * total
            e1 = jnp.exp(cumulative - middle)
            e2 = jnp.exp(cumulative - decay - middle)
            e3 = jnp.exp(middle - cumulative)
            e4 = jnp.exp(middle - cumulative + decay)
            em = jnp.exp(middle)
            et = jnp.exp(total)
            reads = r_ref[here, :].astype(F32)
            values = v_ref[here, :]
            value_wide = spread(values)
            blocks_here.append((b, here))
            for d in range(2):
                left_scale, before_scale, right_scale = (e1, e2, e3) if d == 0 else (e4, e3, e2)
                left = jnp.concatenate([unit * before_scale, reads * left_scale], axis=0)
                chains.append(
                    (d, b, here, left, beta * right_scale, keys * right_scale, em, et, values, value_wide)
                )
        lefts = [c[3] for c in chains]
        keeps = []
        for c in chains:
            strict = below if c[0] == 0 else above
            keeps.append(jnp.concatenate([strict, strict | same], axis=0))
        from_beta = product_all(lefts, [c[4] for c in chains], NT)
        from_beta = [jnp.where(keep, x, 0.0) for keep, x in zip(keeps, from_beta)]
        from_key = product_all(lefts, [c[5] for c in chains], NT)
        from_key = [jnp.where(keep, x, 0.0) for keep, x in zip(keeps, from_key)]
        key_part = [product(x, c[9], None) for x, c in zip(from_key, chains)]
        size, inverse = 1, None
        while size < SPAN:
            corner_mask = (row_t // (2 * size) == col_s // (2 * size)) & (row_t // size != col_s // size)
            corner = [jnp.where(corner_mask, x[:SPAN], 0.0) for x in from_beta]
            if size == 1:
                inverse = [eye - x for x in corner]
            else:
                steps = product_all(corner, inverse)
                steps = product_all(inverse, steps)
                inverse = [x - y for x, y in zip(inverse, steps)]
            size *= 2
        true_left = [c[3] * c[6] for c in chains]
        solved_w = product_all(inverse, [x[:SPAN] for x in true_left])
        solved_v = product_all(inverse, [-x[:SPAN] for x in key_part])
        read = [x[SPAN:] for x in from_beta]
        read_v = product_all(read, solved_v)
        read_w = product_all(read, solved_w)
        on_head = lax.broadcasted_iota(jnp.int32, (width, wide), 0) == lax.rem(
            lane_of((width, wide)), width
        )
        wide_mask = square.astype(F32)
        locals_now = []
        for n, (d, b, here, left, beta_right, key_right, em, et, values, value_wide) in enumerate(chains):
            locals_now.append(key_part[n][SPAN:] + read_v[n])
            readout_s[d, here, :] = true_left[n][SPAN:] - read_w[n]
            beta_high, beta_low = halves(beta_right * em)
            key_high, key_low = halves(key_right * em)
            w_high, w_low = halves(solved_w[n])
            v_high, v_low = halves(solved_v[n])
            beta_three = [beta_high, beta_low, beta_high]
            move = mul(
                jnp.concatenate([w_high, w_high, w_low], axis=0),
                jnp.concatenate(beta_three, axis=0),
                TN,
            )
            put = mul(
                jnp.concatenate([v_high, v_high, v_low, values, values], axis=0),
                jnp.concatenate(beta_three + [key_high, key_low], axis=0),
                TN,
            )
            move = gather_heads(move * wide_mask)
            maps_s[d, b, :width, :] = jnp.where(on_head, et, 0.0) - move
            maps_s[d, b, width:, :] = gather_heads(put * wide_mask)
        for n, (b, here) in enumerate(blocks_here):
            local_s[here, :] = locals_now[2 * n] + locals_now[2 * n + 1]
        return carry

    head_row = lax.broadcasted_iota(jnp.int32, (heads, wide), 0)
    head_hot = (head_row == lane_of((heads, wide)) // width).astype(F32).astype(BF16)
    spike_s[...] = sum(mul(part, head_hot, TN) for part in thirds(spike_ref[...]))

    lax.fori_loop(0, blocks // TOGETHER, each_group, 0)

    first = (
        lax.broadcasted_iota(jnp.int32, (2 * width, wide), 0)
        == lax.rem(lane_of((2 * width, wide)), width)
    ).astype(F32)
    no_rows = jnp.zeros((width, wide), F32)

    def compose(i, carry):
        new = []
        for d in range(2):
            b = i if d == 0 else blocks - 1 - i
            prefix_s[d, b] = carry[d]
            moved = product(carry[d], *spread_pair(maps_s[d, b, :width, :]))
            new.append(moved + jnp.concatenate([no_rows, maps_s[d, b, width:, :]], axis=0))
        return tuple(new)

    whole = lax.fori_loop(0, blocks, compose, (first, first))
    for d in range(2):
        send_maps[d] = whole[d].astype(BF16)
    pl.semaphore_wait(barrier, n_sp - 1 + n_tp - 1)

    experts = meta_ref.shape[1] // 2
    meta_s[tp] = route_table(routes_ref[...], rw_ref[...], experts, capacity, core)

    def meta_copy(d):
        return pltpu.make_async_remote_copy(
            src_ref=meta_s.at[tp],
            dst_ref=meta_s.at[tp],
            send_sem=meta_send.at[d],
            recv_sem=meta_recv.at[tp],
            device_id=(sp, lax.rem(tp + d, n_tp)),
            device_id_type=MESH,
        )

    for d in range(1, n_tp):
        meta_copy(d).start()

    copies = []
    for d in range(1, n_sp):
        target = lax.rem(sp + d, n_sp)
        copy = pltpu.make_async_remote_copy(
            src_ref=send_maps.at[(target < sp).astype(jnp.int32)],
            dst_ref=recv_maps.at[sp],
            send_sem=map_send.at[d],
            recv_sem=map_recv.at[sp],
            device_id=(target, tp),
            device_id_type=MESH,
        )
        copy.start()
        copies.append(copy)
    for d in range(1, n_sp):
        source = lax.rem(sp + d, n_sp)
        pltpu.make_async_remote_copy(
            src_ref=send_maps.at[0],
            dst_ref=recv_maps.at[source],
            send_sem=map_send.at[d],
            recv_sem=map_recv.at[source],
            device_id=(source, tp),
            device_id_type=MESH,
        ).wait_recv()
    for copy in copies:
        copy.wait_send()
    recv_maps[sp] = jnp.zeros((2 * width, wide), BF16)

    def enter(i, carry):
        new = []
        for d in range(2):
            k = i if d == 0 else n_sp - 1 - i
            reached = (k < sp) if d == 0 else (k > sp)
            part = recv_maps[k]
            moved = product(carry[d], spread(part[:width]), None) + part[width:].astype(F32)
            new.append(jnp.where(reached, moved, carry[d]))
        return tuple(new)

    entry = lax.fori_loop(0, n_sp, enter, (no_rows, no_rows))

    gain = gain_ref[...].astype(F32).reshape(1, wide)

    def finish(b, carry):
        here = pl.ds(pl.multiple_of(b * SPAN, SPAN), SPAN)
        mix = local_s[here, :]
        for d in range(2):
            start = product(entry[d], *spread_pair(prefix_s[d, b, :width, :]))
            start = start + prefix_s[d, b, width:, :]
            mix = mix + product(readout_s[d, here, :], *spread_pair(start), dims=NT)
        mean = product(mix, square, None) * (1.0 / width)
        mix = mix - mean
        spread_of = product(mix * mix, square, None) * (1.0 / width)
        mixed = mix * lax.rsqrt(spread_of + GN_EPS) * gain
        mixed_s[here, :] = mixed.astype(BF16)
        return carry

    sibling = (sp, z * 2 + 1 - core)

    def sib_copy(c):
        return pltpu.make_async_remote_copy(
            src_ref=part_s.at[c, pl.ds(pl.multiple_of((1 - core) * rows, rows), rows), :],
            dst_ref=sib_s.at[c],
            send_sem=sib_send.at[c],
            recv_sem=sib_recv.at[c],
            device_id=sibling,
            device_id_type=MESH,
        )

    def z_copy(c):
        return pltpu.make_async_remote_copy(
            src_ref=summed_s.at[c],
            dst_ref=recv_s.at[z],
            send_sem=z_send.at[c],
            recv_sem=z_recv.at[z],
            device_id=(sp, c * 2 + core),
            device_id_type=MESH,
        )

    def chip_at(i):
        return lax.rem(z + 1 + i, n_z)

    def pass_on(i):
        c = chip_at(i)
        sib_copy(c).wait_recv()
        mine = part_s[c, pl.ds(pl.multiple_of(core * rows, rows), rows), :].astype(F32)
        mine = mine + sib_s[c].astype(F32)
        summed_s[c] = mine.astype(BF16)

        @pl.when(c != z)
        def _():
            z_copy(c).start()

    def project(i, carry):
        c = chip_at(i)
        there = pl.ds(pl.multiple_of(c * (2 * rows), 2 * rows), 2 * rows)
        first_block = c * (2 * rows // SPAN)
        lax.fori_loop(first_block, first_block + 2 * rows // SPAN, finish, 0)
        part_s[c] = mul(mixed_s[there, :], w_ref[...]).astype(BF16)
        sib_copy(c).start()

        @pl.when(i > 0)
        def _():
            pass_on(i - 1)

        return carry

    lax.fori_loop(0, n_z, project, 0)
    pass_on(n_z - 1)
    out_ref[...] = summed_s[z].astype(F32)
    for d in range(1, n_z):
        source = lax.rem(z + d, n_z)
        pltpu.make_async_remote_copy(
            src_ref=summed_s.at[source],
            dst_ref=recv_s.at[source],
            send_sem=z_send.at[source],
            recv_sem=z_recv.at[source],
            device_id=(sp, source * 2 + core),
            device_id_type=MESH,
        ).wait_recv()
        out_ref[...] += recv_s[source].astype(F32)
        z_copy(source).wait_send()
    for c in range(n_z):
        sib_copy(c).wait_send()
    for d in range(1, n_tp):
        source = lax.rem(tp + d, n_tp)
        pltpu.make_async_remote_copy(
            src_ref=meta_s.at[tp],
            dst_ref=meta_s.at[source],
            send_sem=meta_send.at[d],
            recv_sem=meta_recv.at[source],
            device_id=(sp, source),
            device_id_type=MESH,
        ).wait_recv()
        meta_copy(d).wait_send()
    meta_ref[...] = meta_s[...]


def mixer(n_sp, n_tp, receptance, keys, values, erase, decay, spike, gain, weight, routes, routing, experts, capacity):
    tokens, wide = keys.shape
    heads = spike.shape[1]
    width = wide // heads
    blocks = tokens // SPAN
    rows = tokens // n_tp
    n_z = n_tp // 2
    model = weight.shape[1]
    vm = pltpu.VMEM
    dma = pltpu.SemaphoreType.DMA
    return pl.pallas_call(
        functools.partial(mixer_kernel, (n_sp, n_tp, heads, capacity)),
        out_shape=[
            jax.ShapeDtypeStruct((rows, model), F32),
            jax.ShapeDtypeStruct((n_tp, 2 * experts, 2 * rows), F32),
        ],
        in_specs=[pl.BlockSpec(memory_space=vm)] * 10,
        out_specs=[pl.BlockSpec(memory_space=vm)] * 2,
        scratch_shapes=[
            vm((tokens, wide), F32),
            vm((tokens, wide), F32),
            vm((2, tokens, wide), F32),
            vm((2, blocks, 2 * width, wide), F32),
            vm((2, blocks, 2 * width, wide), F32),
            vm((2, 2 * width, wide), BF16),
            vm((n_sp, 2 * width, wide), BF16),
            vm((tokens, wide), BF16),
            vm((n_z, 2 * rows, model), BF16),
            vm((n_z, rows, model), BF16),
            vm((n_z, rows, model), BF16),
            vm((n_z, rows, model), BF16),
            vm((n_tp, 2 * experts, 2 * rows), F32),
            dma((n_tp,)),
            dma((n_tp,)),
            dma((n_sp,)),
            dma((n_sp,)),
            dma((n_z,)),
            dma((n_z,)),
            dma((n_z,)),
            dma((n_z,)),
        ],
        compiler_params=pltpu.CompilerParams(
            collective_id=0, has_side_effects=True, vmem_limit_bytes=56 * 1024 * 1024
        ),
        cost_estimate=pl.CostEstimate(flops=10**10, bytes_accessed=10**7, transcendentals=0),
    )(receptance, keys, values, erase, decay, spike.T, gain, weight, routes.T, routing.T)


def expert_kernel(
    geometry,
    input_ref, projected_ref, gain_ref, meta_ref, gate_hbm, up_hbm, down_hbm,
    shared_gate_hbm, shared_up_hbm, shared_down_hbm, out_ref,
    gate, up, down, shared_gate, shared_up, shared_down,
    residual, table, own, xg, sel_out, sel_in, y_buf, y_sib, sh_buf, sh_sib,
    q_out, q_in, t_out, t_in, fin, fin_sib,
    w_sem, own_sem, z_send, z_recv, xr_send, xr_recv, sel_send, sel_recv, sr_send, sr_recv,
    y_send, y_recv, sh_send, sh_recv, q_send, q_recv, t_send, t_recv, fin_sem,
):
    n_sp, n_tp, capacity = geometry
    n_z = n_tp // 2
    rows, model = input_ref.shape
    half = model // 2
    pair = 2 * rows
    slots = 2 * capacity
    local = gate_hbm.shape[0]
    experts = meta_ref.shape[1] // 2
    hidden = gate_hbm.shape[2]
    sp, tp = lax.axis_index("sp"), lax.axis_index("tp")
    z, core = tp // 2, lax.rem(tp, 2)
    other = 1 - core
    sibling = (sp, z * 2 + other)

    barrier = pltpu.get_barrier_semaphore()
    for d in range(1, n_sp):
        pl.semaphore_signal(barrier, inc=1, device_id=(lax.rem(sp + d, n_sp), tp), device_id_type=MESH)
    for d in range(1, n_z):
        pl.semaphore_signal(
            barrier, inc=1, device_id=(sp, lax.rem(z + d, n_z) * 2 + core), device_id_type=MESH
        )
    pl.semaphore_signal(barrier, inc=1, device_id=sibling, device_id_type=MESH)

    loads = [
        pltpu.make_async_copy(source, target, w_sem.at[i])
        for i, (source, target) in enumerate(
            [
                (gate_hbm, gate), (up_hbm, up), (down_hbm, down), (shared_gate_hbm, shared_gate),
                (shared_up_hbm, shared_up), (shared_down_hbm, shared_down),
            ]
        )
    ]
    for load in loads:
        load.start()

    def remote(source, target, send, recv, device):
        return pltpu.make_async_remote_copy(
            src_ref=source, dst_ref=target, send_sem=send, recv_sem=recv,
            device_id=device, device_id_type=MESH,
        )

    def rows_at(c):
        return pl.ds(pl.multiple_of(c * rows, rows), rows)

    total = input_ref[...].astype(F32) + projected_ref[...]
    residual[...] = total
    normed = total * lax.rsqrt(jnp.mean(total * total, axis=-1, keepdims=True) + RMS_EPS)
    normed = (normed * gain_ref[...].astype(F32).reshape(1, model)).astype(BF16)
    for h in range(2):
        own[h] = normed[:, h * half : (h + 1) * half]
        xg[z, h, rows_at(core), :] = normed[:, h * half : (h + 1) * half]
    for c in range(n_z):
        table[c] = meta_ref[2 * c] + meta_ref[2 * c + 1]
    pl.semaphore_wait(barrier, n_sp - 1 + n_z)

    own_copy = remote(own, xg.at[z, :, rows_at(core), :], own_sem.at[0], own_sem.at[1], sibling)
    own_copy.start()
    own_copy.wait_recv()

    def z_copy(c, target):
        return remote(xg.at[c, core], xg.at[c, core], z_send.at[target], z_recv.at[c], (sp, target * 2 + core))

    for d in range(1, n_z):
        z_copy(z, lax.rem(z + n_z - d, n_z)).start()

    def relay_x(c):
        return remote(xg.at[c, core], xg.at[c, core], xr_send.at[c], xr_recv.at[c], sibling)

    def relay_x_in(c):
        return remote(xg.at[c, other], xg.at[c, other], xr_send.at[c], xr_recv.at[c], sibling)

    def sel_copy(c, g):
        return remote(
            sel_out.at[c, g], sel_in.at[c, core, :, sp], sel_send.at[c, g], sel_recv.at[c, sp],
            (g, tp),
        )

    def sel_arrival(c, g):
        return remote(
            sel_out.at[c, g], sel_in.at[c, core, :, g], sel_send.at[c, g], sel_recv.at[c, g], (g, tp)
        )

    def relay_sel(c, g):
        there = sel_in.at[c, core, :, g]
        return remote(there, there, sr_send.at[c, g], sr_recv.at[c, g], sibling)

    def relay_sel_in(c, g):
        there = sel_in.at[c, other, :, g]
        return remote(there, there, sr_send.at[c, g], sr_recv.at[c, g], sibling)

    slot_ids = (lax.broadcasted_iota(jnp.int32, (slots, pair), 0) + 1).astype(F32)

    def picks(c, g):
        return [(slot_ids == table[c, pl.ds(g * local + j, 1), :]).astype(F32) for j in range(local)]

    def select(c, g, h):
        chosen = jnp.concatenate(picks(c, g), axis=0).astype(BF16)
        return mul(chosen, xg[c, h]).astype(BF16).reshape(local, slots, half)

    def send_rows(c):
        for d in range(1, n_sp):
            g = lax.rem(sp + d, n_sp)
            sel_out[c, g] = select(c, g, core)
            sel_copy(c, g).start()

    send_rows(z)
    for load in loads:
        load.wait()

    def feed(x, first, second):
        gate_value = mul(x[0], first[:half, :]) + mul(x[1], first[half:, :])
        up_value = mul(x[0], second[:half, :]) + mul(x[1], second[half:, :])
        return (jax.nn.silu(gate_value) * up_value).astype(BF16)

    def y_copy(c):
        return remote(y_buf.at[c, other], y_sib.at[c], y_send.at[c], y_recv.at[c], sibling)

    def sh_copy(c):
        return remote(sh_buf.at[c, other], sh_sib.at[c], sh_send.at[c], sh_recv.at[c], sibling)

    def q_copy(c, g):
        return remote(q_out.at[c, :, g], q_in.at[c, :, sp], q_send.at[c, g], q_recv.at[c, sp], (g, tp))

    def q_arrival(c, g):
        return remote(q_out.at[c, :, g], q_in.at[c, :, g], q_send.at[c, g], q_recv.at[c, g], (g, tp))

    def t_copy(c):
        return remote(t_out.at[c], t_in.at[z], t_send.at[c], t_recv.at[z], (sp, c * 2 + core))

    def t_arrival(c):
        return remote(t_out.at[c], t_in.at[c], t_send.at[c], t_recv.at[c], (sp, c * 2 + core))

    def combine(c):
        for d in range(1, n_sp):
            q_arrival(c, lax.rem(sp + d, n_sp)).wait_recv()
        result = sh_buf[c, core].astype(F32) + sh_sib[c].astype(F32)
        for j in range(local):
            weighted = []
            for g in range(n_sp):
                hot = slot_ids == table[c, g * local + j : g * local + j + 1, :]
                weight = table[c, experts + g * local + j : experts + g * local + j + 1, :]
                weighted.append(jnp.where(hot, weight, 0.0))
            high, low = halves(jnp.concatenate(weighted, axis=0))
            values = q_in[c, j].reshape(n_sp * slots, half)
            result = result + mul(high, values, TN) + mul(low, values, TN)
        return result

    def pass_on(c):
        t_out[c] = combine(c).astype(BF16)
        t_copy(c).start()

    def step(k, carry):
        c = lax.rem(z + k, n_z)

        @pl.when(k < n_z - 1)
        def _():
            later = lax.rem(z + k + 1, n_z)
            z_copy(later, z).wait_recv()
            relay_x(later).start()
            send_rows(later)

        for d in range(1, n_sp):
            g = lax.rem(sp + n_sp - d, n_sp)
            sel_arrival(c, g).wait_recv()
            relay_sel(c, g).start()

        @pl.when(k > 0)
        def _():
            relay_x_in(c).wait_recv()

        for h in range(2):
            sel_in[c, h, :, sp] = select(c, sp, h)
        hidden_rows = feed([xg[c, 0], xg[c, 1]], shared_gate, shared_up)
        for h in range(2):
            sh_buf[c, h] = mul(hidden_rows, shared_down[:, h * half : (h + 1) * half]).astype(BF16)
        sh_copy(c).start()
        for d in range(1, n_sp):
            relay_sel_in(c, lax.rem(sp + n_sp - d, n_sp)).wait_recv()
        for j in range(local):
            x = [sel_in[c, h, j].reshape(n_sp * slots, half) for h in range(2)]
            hidden_rows = feed(x, gate.at[j], up.at[j])
            for h in range(2):
                y = mul(hidden_rows, down[j, :, h * half : (h + 1) * half]).astype(BF16)
                y_buf[c, h, j] = y.reshape(n_sp, slots, half)
        y_copy(c).start()

        @pl.when(k > 1)
        def _():
            pass_on(lax.rem(z + k - 1, n_z))

        y_copy(c).wait_recv()
        sh_copy(c).wait_recv()
        q_out[c] = (y_buf[c, core].astype(F32) + y_sib[c].astype(F32)).astype(BF16)
        q_in[c, :, sp] = q_out[c, :, sp]
        for d in range(1, n_sp):
            q_copy(c, lax.rem(sp + d, n_sp)).start()
        return carry

    lax.fori_loop(0, n_z, step, 0)
    pass_on(lax.rem(z + n_z - 1, n_z))
    fin[...] = combine(z)
    for d in range(1, n_z):
        c = lax.rem(z + d, n_z)
        t_arrival(c).wait_recv()
        fin[...] += t_in[c].astype(F32)
    fin_copy = remote(fin.at[rows_at(other), :], fin_sib, fin_sem.at[0], fin_sem.at[1], sibling)
    fin_copy.start()

    def columns(c):
        return pl.ds(pl.multiple_of(c * half, half), half)

    mine = residual[:, columns(core)] + fin[rows_at(core), :]
    out_ref[:, columns(core)] = mine.astype(out_ref.dtype)
    fin_copy.wait_recv()
    theirs = residual[:, columns(other)] + fin_sib[...]
    out_ref[:, columns(other)] = theirs.astype(out_ref.dtype)
    fin_copy.wait_send()
    own_copy.wait_send()
    for c in range(n_z):
        y_copy(c).wait_send()
        sh_copy(c).wait_send()
        for d in range(1, n_sp):
            g = lax.rem(sp + d, n_sp)
            sel_copy(c, g).wait_send()
            relay_sel(c, g).wait_send()
            q_copy(c, g).wait_send()
    for d in range(1, n_z):
        c = lax.rem(z + d, n_z)
        z_copy(z, c).wait_send()
        relay_x(c).wait_send()
        t_copy(c).wait_send()


def expert_shapes(n_sp, n_tp, rows, model, local, hidden, experts, capacity):
    n_z, half, pair, slots = n_tp // 2, model // 2, 2 * rows, 2 * capacity
    return [
        ((local, model, hidden), BF16),
        ((local, model, hidden), BF16),
        ((local, hidden, model), BF16),
        ((model, hidden), BF16),
        ((model, hidden), BF16),
        ((hidden, model), BF16),
        ((rows, model), F32),
        ((n_z, 2 * experts, pair), F32),
        ((2, rows, half), BF16),
        ((n_z, 2, pair, half), BF16),
        ((n_z, n_sp, local, slots, half), BF16),
        ((n_z, 2, local, n_sp, slots, half), BF16),
        ((n_z, 2, local, n_sp, slots, half), BF16),
        ((n_z, local, n_sp, slots, half), BF16),
        ((n_z, 2, pair, half), BF16),
        ((n_z, pair, half), BF16),
        ((n_z, local, n_sp, slots, half), BF16),
        ((n_z, local, n_sp, slots, half), BF16),
        ((n_z, pair, half), BF16),
        ((n_z, pair, half), BF16),
        ((pair, half), F32),
        ((rows, half), F32),
    ]


def expert_layer(
    n_sp, n_tp, shapes, capacity, layer_input, projected, gain, meta, gate, up, down,
    shared_gate, shared_up, shared_down,
):
    n_z = n_tp // 2
    vm = pltpu.VMEM
    dma = pltpu.SemaphoreType.DMA
    inside, outside = pl.BlockSpec(memory_space=vm), pl.BlockSpec(memory_space=pl.ANY)
    one, two = dma((n_z,)), dma((n_z, n_sp))
    return pl.pallas_call(
        functools.partial(expert_kernel, (n_sp, n_tp, capacity)),
        out_shape=jax.ShapeDtypeStruct(layer_input.shape, BF16),
        in_specs=[inside] * 4 + [outside] * 6,
        out_specs=inside,
        scratch_shapes=[vm(shape, dtype) for shape, dtype in shapes]
        + [dma((6,)), dma((2,)), one, one, one, one, two, two, two, two]
        + [one, one, one, one, two, two, one, one, dma((2,))],
        compiler_params=pltpu.CompilerParams(
            collective_id=1, has_side_effects=True, vmem_limit_bytes=VMEM_LIMIT
        ),
        cost_estimate=pl.CostEstimate(flops=10**10, bytes_accessed=10**7, transcendentals=0),
    )(
        layer_input, projected, gain, meta, gate, up, down,
        shared_gate, shared_up, shared_down,
    )


highest = lax.Precision.HIGHEST


def body(
    layer_input,
    receptance,
    keys,
    values,
    erase_preact,
    decay_preact,
    decay_spike,
    head_norm_gain,
    output_weight,
    expert_norm_gain,
    routes,
    routing_weight,
    expert_gate_weight,
    expert_up_weight,
    expert_down_weight,
    shared_gate_weight,
    shared_up_weight,
    shared_down_weight,
):
    row_count, model_width = layer_input.shape
    top_count = routes.shape[1]
    expert_local = expert_gate_weight.shape[0]
    sp_count, tp_count = lax.axis_size("sp"), lax.axis_size("tp")
    expert_total = expert_local * sp_count
    capacity = max(2, (3 * row_count * top_count + 2 * expert_total - 1) // (2 * expert_total))
    slot_total = sp_count * capacity * expert_local
    projected, meta = mixer(
        sp_count, tp_count, receptance, keys, values, erase_preact, decay_preact, decay_spike,
        head_norm_gain, output_weight, routes, routing_weight, expert_total, capacity,
    )
    shapes = expert_shapes(
        sp_count, tp_count, row_count, model_width, expert_local, expert_gate_weight.shape[2],
        expert_total, capacity,
    )
    used = sum(math.prod(shape) * jnp.dtype(dtype).itemsize for shape, dtype in shapes)
    if used < VMEM_LIMIT * 7 // 8 and (2 * capacity) % 16 == 0:
        return expert_layer(
            sp_count, tp_count, shapes, capacity, layer_input, projected, expert_norm_gain, meta,
            expert_gate_weight, expert_up_weight, expert_down_weight,
            shared_gate_weight, shared_up_weight, shared_down_weight,
        )
    residual = layer_input.astype(jnp.float32) + projected
    normed = residual * lax.rsqrt(jnp.mean(residual * residual, axis=-1, keepdims=True) + RMS_EPS)
    normed = (normed * expert_norm_gain.astype(jnp.float32)).astype(jnp.bfloat16)
    everyone = lax.all_gather(normed, "tp", axis=0, tiled=True)
    entries = routes.reshape(-1)
    entry_count = entries.shape[0]
    expert_hot = (entries[:, None] == lax.broadcasted_iota(jnp.int32, (1, expert_total), 1)).astype(
        jnp.int32
    )
    rank_in = jnp.sum((jnp.cumsum(expert_hot, axis=0) - 1) * expert_hot, axis=1)
    slot_of = entries * capacity + rank_in
    slot_hot = (slot_of[:, None] == lax.broadcasted_iota(jnp.int32, (1, slot_total), 1)).astype(
        jnp.float32
    )
    owner_hot = (
        lax.broadcasted_iota(jnp.int32, (entry_count, 1), 0) // top_count
        == lax.broadcasted_iota(jnp.int32, (1, row_count), 1)
    ).astype(jnp.float32)
    placing = jnp.dot(slot_hot.T, owner_hot, precision=highest)
    weighting = jnp.dot(owner_hot.T, slot_hot * routing_weight.reshape(-1, 1), precision=highest)
    outgoing = jnp.dot(placing.astype(jnp.bfloat16), normed, preferred_element_type=jnp.float32)
    outgoing = outgoing.astype(jnp.bfloat16).reshape(sp_count, expert_local, capacity, model_width)
    arrived = lax.all_to_all(outgoing, "sp", split_axis=0, concat_axis=0, tiled=True)

    def gathered(rows):
        return lax.all_gather(rows, "tp", axis=0, tiled=True)

    def hidden_layer(rows, gate, up, down):
        gate_value = jnp.dot(rows, gate, preferred_element_type=jnp.float32)
        up_value = jnp.dot(rows, up, preferred_element_type=jnp.float32)
        hidden = (jax.nn.silu(gate_value) * up_value).astype(jnp.bfloat16)
        partial_rows = jnp.dot(hidden, down, preferred_element_type=jnp.float32)
        return lax.psum_scatter(
            partial_rows.astype(jnp.bfloat16), "tp", scatter_dimension=0, tiled=True
        )

    shared = hidden_layer(everyone, shared_gate_weight, shared_up_weight, shared_down_weight)
    routed_rows = []
    for j in range(expert_local):
        rows = gathered(arrived[:, j].reshape(sp_count * capacity, model_width))
        out = hidden_layer(
            rows, expert_gate_weight[j], expert_up_weight[j], expert_down_weight[j]
        )
        routed_rows.append(out.reshape(sp_count, 1, capacity, model_width))
    routed_rows = jnp.concatenate(routed_rows, axis=1)
    returned = lax.all_to_all(routed_rows, "sp", split_axis=0, concat_axis=0, tiled=True)
    routed = jnp.dot(
        weighting, returned.reshape(slot_total, model_width).astype(jnp.float32), precision=highest
    )
    return (residual + shared.astype(jnp.float32) + routed).astype(jnp.bfloat16)


def solution(mesh):
    return jax.shard_map(
        body,
        mesh=mesh,
        in_specs=(
            P(("sp", "tp"), None),
            P("sp", "tp"),
            P("sp", "tp"),
            P("sp", "tp"),
            P("sp", "tp"),
            P("sp", "tp"),
            P("sp", "tp"),
            P("tp"),
            P("tp", None),
            P(),
            P(("sp", "tp"), None),
            P(("sp", "tp"), None),
            P("sp", None, "tp"),
            P("sp", None, "tp"),
            P("sp", "tp", None),
            P(None, "tp"),
            P(None, "tp"),
            P("tp", None),
        ),
        out_specs=P(("sp", "tp"), None),
        check_vma=False,
    )
```

```python
import functools
import math
import jax
import jax.numpy as jnp
from jax import lax
from jax.experimental import pallas as pl
from jax.experimental.pallas import tpu as pltpu
from jax.sharding import PartitionSpec as P

SPAN = 64
TOGETHER = 4
VMEM_LIMIT = 67043328
GN_EPS = 0.00064
RMS_EPS = 1e-06
F32, BF16 = jnp.float32, jnp.bfloat16
MESH = pl.DeviceIdType.MESH
NN = (((1,), (0,)), ((), ()))
NT = (((1,), (1,)), ((), ()))
TN = (((0,), (0,)), ((), ()))


def mul(left, right, dims=NN):
    return lax.dot_general(left, right, dims, preferred_element_type=F32)


def halves(x):
    high = x.astype(BF16)
    return high, (x - high.astype(F32)).astype(BF16)


def thirds(x):
    first = x.astype(BF16)
    rest = x - first.astype(F32)
    second = rest.astype(BF16)
    return first, second, (rest - second.astype(F32)).astype(BF16)


def product(left, right_high, right_low, dims=NN):
    rows = left.shape[0]
    high, low = halves(left)
    both = mul(jnp.concatenate([high, low], axis=0), right_high, dims)
    out = both[:rows] + both[rows:]
    if right_low is not None:
        out = out + mul(high, right_low, dims)
    return out


def near_order(n_z):
    table = []
    for z in range(n_z):
        others = sorted((c for c in range(n_z) if c != z), key=lambda c: (abs(c - z), c))
        table.append(others + [z])
    return table


def out_order(n_z):
    return [line[1:-1] + line[:1] + line[-1:] for line in near_order(n_z)]


def far_order(n_z):
    table = []
    for z in range(n_z):
        others = sorted((c for c in range(n_z) if c != z), key=lambda c: (-abs(c - z), c))
        table.append(others + [z])
    return table


def pick(table, z, k):
    found = jnp.int32(0)
    for i, line in enumerate(table):
        for j, value in enumerate(line):
            found = found + value * ((z == i) & (k == j)).astype(jnp.int32)
    return found


def route_table(routes, weights, experts, capacity, core):
    top, rows = routes.shape
    lines = lax.broadcasted_iota(jnp.int32, (experts, rows), 0)
    hot = jnp.zeros((experts, rows), F32)
    weight = jnp.zeros((experts, rows), F32)
    for j in range(top):
        chosen = routes[j : j + 1, :] == lines
        hot = hot + chosen.astype(F32)
        weight = weight + jnp.where(chosen, weights[j : j + 1, :], 0.0)
    row = lax.broadcasted_iota(jnp.int32, (rows, rows), 0)
    col = lax.broadcasted_iota(jnp.int32, (rows, rows), 1)
    rank = mul(hot.astype(BF16), (row < col).astype(F32).astype(BF16))
    place = (rank + 1.0 + (core * capacity).astype(F32)) * hot
    own = lax.broadcasted_iota(jnp.int32, (rows, 2 * rows), 0) + core * rows
    shifted = (own == lax.broadcasted_iota(jnp.int32, (rows, 2 * rows), 1)).astype(F32).astype(BF16)
    placed = mul(place.astype(BF16), shifted)
    weighed = sum(mul(part, shifted) for part in thirds(weight))
    return jnp.concatenate([placed, weighed], axis=0)


def mixer_kernel(
    geometry,
    r_ref, k_ref, v_ref, e_ref, dp_ref, spike_ref, gain_ref, w_ref, routes_ref, rw_ref,
    out_ref, meta_ref,
    spike_s, local_s, readout_s, maps_s, prefix_s, send_maps, recv_maps,
    mixed_s, part_s, sib_s, summed_s, recv_s,
    meta_s, meta_send, meta_recv, map_send, map_recv, sib_send, sib_recv, z_send, z_recv,
):
    n_sp, n_tp, heads, capacity = geometry
    n_z = n_tp // 2
    tokens, wide = k_ref.shape
    width = wide // heads
    blocks = tokens // SPAN
    rows = tokens // n_tp
    sp, tp = lax.axis_index("sp"), lax.axis_index("tp")
    z, core = tp // 2, lax.rem(tp, 2)

    barrier = pltpu.get_barrier_semaphore()
    for d in range(1, n_sp):
        pl.semaphore_signal(barrier, inc=1, device_id=(lax.rem(sp + d, n_sp), tp), device_id_type=MESH)
    for d in range(1, n_tp):
        pl.semaphore_signal(barrier, inc=1, device_id=(sp, lax.rem(tp + d, n_tp)), device_id_type=MESH)

    def head_mask(shape, dtype):
        first = lax.broadcasted_iota(jnp.int32, shape, 0) // width
        second = lax.broadcasted_iota(jnp.int32, shape, 1) // width
        return (first == second).astype(F32).astype(dtype)

    square = head_mask((wide, wide), BF16)

    def spread(x):
        return jnp.concatenate([x] * heads, axis=0) * square

    def spread_pair(x):
        high, low = halves(x)
        return spread(high), spread(low)

    def gather_heads(x):
        total = x[:width]
        for h in range(1, heads):
            total = total + x[h * width : (h + 1) * width]
        return total

    def lane_of(shape):
        return lax.broadcasted_iota(jnp.int32, shape, 1)

    row_t = lax.broadcasted_iota(jnp.int32, (SPAN, wide), 0)
    col_s = lax.rem(lane_of((SPAN, wide)), SPAN)
    below = row_t > col_s
    above = row_t < col_s
    same = row_t == col_s
    tri = (
        lax.broadcasted_iota(jnp.int32, (SPAN, SPAN), 0)
        >= lax.broadcasted_iota(jnp.int32, (SPAN, SPAN), 1)
    ).astype(F32).astype(BF16)
    tri3 = jnp.concatenate([tri, tri, tri], axis=1)
    eye = same.astype(F32)

    def product_all(lefts, rights, dims=NN):
        pairs = [spread_pair(right) for right in rights]
        return [product(left, *pair, dims=dims) for left, pair in zip(lefts, pairs)]

    def each_group(i, carry):
        chains = []
        blocks_here = []
        for b in [i * TOGETHER + n for n in range(TOGETHER)]:
            here = pl.ds(pl.multiple_of(b * SPAN, SPAN), SPAN)
            keys = k_ref[here, :].astype(F32)
            square_high, square_low = halves(keys * keys)
            norm = mul(jnp.concatenate([square_high, square_low], axis=0), square)
            norm = norm[:SPAN] + norm[SPAN:]
            unit = keys * lax.rsqrt(norm + 1e-06)
            beta = unit * jax.nn.sigmoid(e_ref[here, :].astype(F32))
            decay = -0.6065306597126334 * jax.nn.sigmoid(dp_ref[here, :].astype(F32))
            decay = decay + spike_s[here, :]
            decay_1, decay_2, decay_3 = thirds(decay)
            cumulative = mul(tri3, jnp.concatenate([decay_1, decay_2, decay_3], axis=0))
            total = cumulative[SPAN - 1 : SPAN, :]
            middle = 0.5 * total
            e1 = jnp.exp(cumulative - middle)
            e2 = jnp.exp(cumulative - decay - middle)
            e3 = jnp.exp(middle - cumulative)
            e4 = jnp.exp(middle - cumulative + decay)
            em = jnp.exp(middle)
            et = jnp.exp(total)
            reads = r_ref[here, :].astype(F32)
            values = v_ref[here, :]
            value_wide = spread(values)
            blocks_here.append((b, here))
            for d in range(2):
                left_scale, before_scale, right_scale = (e1, e2, e3) if d == 0 else (e4, e3, e2)
                left = jnp.concatenate([unit * before_scale, reads * left_scale], axis=0)
                chains.append(
                    (d, b, here, left, beta * right_scale, keys * right_scale, em, et, values, value_wide)
                )
        lefts = [c[3] for c in chains]
        keeps = []
        for c in chains:
            strict = below if c[0] == 0 else above
            keeps.append(jnp.concatenate([strict, strict | same], axis=0))
        from_beta = product_all(lefts, [c[4] for c in chains], NT)
        from_beta = [jnp.where(keep, x, 0.0) for keep, x in zip(keeps, from_beta)]
        from_key = product_all(lefts, [c[5] for c in chains], NT)
        from_key = [jnp.where(keep, x, 0.0) for keep, x in zip(keeps, from_key)]
        key_part = [product(x, c[9], None) for x, c in zip(from_key, chains)]
        size, inverse = 1, None
        while size < SPAN:
            corner_mask = (row_t // (2 * size) == col_s // (2 * size)) & (row_t // size != col_s // size)
            corner = [jnp.where(corner_mask, x[:SPAN], 0.0) for x in from_beta]
            if size == 1:
                inverse = [eye - x for x in corner]
            else:
                steps = product_all(corner, inverse)
                steps = product_all(inverse, steps)
                inverse = [x - y for x, y in zip(inverse, steps)]
            size *= 2
        true_left = [c[3] * c[6] for c in chains]
        solved_w = product_all(inverse, [x[:SPAN] for x in true_left])
        solved_v = product_all(inverse, [-x[:SPAN] for x in key_part])
        read = [x[SPAN:] for x in from_beta]
        read_v = product_all(read, solved_v)
        read_w = product_all(read, solved_w)
        on_head = lax.broadcasted_iota(jnp.int32, (width, wide), 0) == lax.rem(
            lane_of((width, wide)), width
        )
        wide_mask = square.astype(F32)
        locals_now = []
        for n, (d, b, here, left, beta_right, key_right, em, et, values, value_wide) in enumerate(chains):
            locals_now.append(key_part[n][SPAN:] + read_v[n])
            readout_s[d, here, :] = true_left[n][SPAN:] - read_w[n]
            beta_high, beta_low = halves(beta_right * em)
            key_high, key_low = halves(key_right * em)
            w_high, w_low = halves(solved_w[n])
            v_high, v_low = halves(solved_v[n])
            beta_three = [beta_high, beta_low, beta_high]
            move = mul(
                jnp.concatenate([w_high, w_high, w_low], axis=0),
                jnp.concatenate(beta_three, axis=0),
                TN,
            )
            put = mul(
                jnp.concatenate([v_high, v_high, v_low, values, values], axis=0),
                jnp.concatenate(beta_three + [key_high, key_low], axis=0),
                TN,
            )
            move = gather_heads(move * wide_mask)
            maps_s[d, b, :width, :] = jnp.where(on_head, et, 0.0) - move
            maps_s[d, b, width:, :] = gather_heads(put * wide_mask)
        for n, (b, here) in enumerate(blocks_here):
            local_s[here, :] = locals_now[2 * n] + locals_now[2 * n + 1]
        return carry

    head_row = lax.broadcasted_iota(jnp.int32, (heads, wide), 0)
    head_hot = (head_row == lane_of((heads, wide)) // width).astype(F32).astype(BF16)
    spike_s[...] = sum(mul(part, head_hot, TN) for part in thirds(spike_ref[...]))

    lax.fori_loop(0, blocks // TOGETHER, each_group, 0)

    first = (
        lax.broadcasted_iota(jnp.int32, (2 * width, wide), 0)
        == lax.rem(lane_of((2 * width, wide)), width)
    ).astype(F32)
    no_rows = jnp.zeros((width, wide), F32)

    def compose(i, carry):
        new = []
        for d in range(2):
            b = i if d == 0 else blocks - 1 - i
            prefix_s[d, b] = carry[d]
            moved = product(carry[d], *spread_pair(maps_s[d, b, :width, :]))
            new.append(moved + jnp.concatenate([no_rows, maps_s[d, b, width:, :]], axis=0))
        return tuple(new)

    whole = lax.fori_loop(0, blocks, compose, (first, first))
    for d in range(2):
        send_maps[d] = whole[d].astype(BF16)
    pl.semaphore_wait(barrier, n_sp - 1 + n_tp - 1)

    experts = meta_ref.shape[1] // 2
    meta_s[tp] = route_table(routes_ref[...], rw_ref[...], experts, capacity, core)

    def meta_copy(d):
        return pltpu.make_async_remote_copy(
            src_ref=meta_s.at[tp],
            dst_ref=meta_s.at[tp],
            send_sem=meta_send.at[d],
            recv_sem=meta_recv.at[tp],
            device_id=(sp, lax.rem(tp + d, n_tp)),
            device_id_type=MESH,
        )

    for d in range(1, n_tp):
        meta_copy(d).start()

    copies = []
    for d in range(1, n_sp):
        target = lax.rem(sp + d, n_sp)
        copy = pltpu.make_async_remote_copy(
            src_ref=send_maps.at[(target < sp).astype(jnp.int32)],
            dst_ref=recv_maps.at[sp],
            send_sem=map_send.at[d],
            recv_sem=map_recv.at[sp],
            device_id=(target, tp),
            device_id_type=MESH,
        )
        copy.start()
        copies.append(copy)
    for d in range(1, n_sp):
        source = lax.rem(sp + d, n_sp)
        pltpu.make_async_remote_copy(
            src_ref=send_maps.at[0],
            dst_ref=recv_maps.at[source],
            send_sem=map_send.at[d],
            recv_sem=map_recv.at[source],
            device_id=(source, tp),
            device_id_type=MESH,
        ).wait_recv()
    for copy in copies:
        copy.wait_send()
    recv_maps[sp] = jnp.zeros((2 * width, wide), BF16)

    def enter(i, carry):
        new = []
        for d in range(2):
            k = i if d == 0 else n_sp - 1 - i
            reached = (k < sp) if d == 0 else (k > sp)
            part = recv_maps[k]
            moved = product(carry[d], spread(part[:width]), None) + part[width:].astype(F32)
            new.append(jnp.where(reached, moved, carry[d]))
        return tuple(new)

    entry = lax.fori_loop(0, n_sp, enter, (no_rows, no_rows))

    gain = gain_ref[...].astype(F32).reshape(1, wide)

    def finish(b, carry):
        here = pl.ds(pl.multiple_of(b * SPAN, SPAN), SPAN)
        mix = local_s[here, :]
        for d in range(2):
            start = product(entry[d], *spread_pair(prefix_s[d, b, :width, :]))
            start = start + prefix_s[d, b, width:, :]
            mix = mix + product(readout_s[d, here, :], *spread_pair(start), dims=NT)
        mean = product(mix, square, None) * (1.0 / width)
        mix = mix - mean
        spread_of = product(mix * mix, square, None) * (1.0 / width)
        mixed = mix * lax.rsqrt(spread_of + GN_EPS) * gain
        mixed_s[here, :] = mixed.astype(BF16)
        return carry

    sibling = (sp, z * 2 + 1 - core)

    def sib_copy(c):
        return pltpu.make_async_remote_copy(
            src_ref=part_s.at[c, pl.ds(pl.multiple_of((1 - core) * rows, rows), rows), :],
            dst_ref=sib_s.at[c],
            send_sem=sib_send.at[c],
            recv_sem=sib_recv.at[c],
            device_id=sibling,
            device_id_type=MESH,
        )

    low_end = ((z == 0) & (n_z > 2)).astype(jnp.int32)
    high_end = ((z == n_z - 1) & (n_z > 2)).astype(jnp.int32)
    at_end = low_end + high_end
    inner = low_end + high_end * (n_z - 2)

    def z_copy(c):
        through = at_end * (c != inner).astype(jnp.int32)
        slot = through * (n_z + c) + (1 - through) * z
        target = at_end * inner + (1 - at_end) * c
        return pltpu.make_async_remote_copy(
            src_ref=summed_s.at[c],
            dst_ref=recv_s.at[slot],
            send_sem=z_send.at[c],
            recv_sem=z_recv.at[slot],
            device_id=(sp, target * 2 + core),
            device_id_type=MESH,
        )

    def arrival(slot):
        return pltpu.make_async_remote_copy(
            src_ref=summed_s.at[0],
            dst_ref=recv_s.at[slot],
            send_sem=z_send.at[0],
            recv_sem=z_recv.at[slot],
            device_id=sibling,
            device_id_type=MESH,
        )

    def joins(c):
        return (n_z > 2) & (((z == 1) & (c > 1)) | ((z == n_z - 2) & (c < n_z - 2)))

    far = far_order(n_z)

    def chip_at(i):
        return pick(far, z, i)

    def pass_on(i):
        c = chip_at(i)
        sib_copy(c).wait_recv()
        mine = part_s[c, pl.ds(pl.multiple_of(core * rows, rows), rows), :].astype(F32)
        mine = mine + sib_s[c].astype(F32)
        summed_s[c] = mine.astype(BF16)

        @pl.when((c != z) & jnp.logical_not(joins(c)))
        def _():
            z_copy(c).start()

    def project(i, carry):
        c = chip_at(i)
        there = pl.ds(pl.multiple_of(c * (2 * rows), 2 * rows), 2 * rows)
        first_block = c * (2 * rows // SPAN)
        lax.fori_loop(first_block, first_block + 2 * rows // SPAN, finish, 0)
        part_s[c] = mul(mixed_s[there, :], w_ref[...]).astype(BF16)
        sib_copy(c).start()

        @pl.when(i > 0)
        def _():
            pass_on(i - 1)

        return carry

    lax.fori_loop(0, n_z, project, 0)
    pass_on(n_z - 1)
    for i in range(n_z - 1):
        c = chip_at(i)

        @pl.when(joins(c))
        def _():
            arrival(n_z + c).wait_recv()
            summed_s[c] = (summed_s[c].astype(F32) + recv_s[n_z + c].astype(F32)).astype(BF16)
            z_copy(c).start()

    out_ref[...] = summed_s[z].astype(F32)
    for source in range(n_z):
        direct = z != source
        if n_z > 2 and source == 0:
            direct = z == 1
        if n_z > 2 and source == n_z - 1:
            direct = z == n_z - 2

        @pl.when(direct)
        def _():
            arrival(source).wait_recv()
            out_ref[...] += recv_s[source].astype(F32)

    for d in range(1, n_z):
        z_copy(lax.rem(z + d, n_z)).wait_send()
    for c in range(n_z):
        sib_copy(c).wait_send()
    for d in range(1, n_tp):
        source = lax.rem(tp + d, n_tp)
        pltpu.make_async_remote_copy(
            src_ref=meta_s.at[tp],
            dst_ref=meta_s.at[source],
            send_sem=meta_send.at[d],
            recv_sem=meta_recv.at[source],
            device_id=(sp, source),
            device_id_type=MESH,
        ).wait_recv()
        meta_copy(d).wait_send()
    meta_ref[...] = meta_s[...]


def mixer(n_sp, n_tp, receptance, keys, values, erase, decay, spike, gain, weight, routes, routing, experts, capacity):
    tokens, wide = keys.shape
    heads = spike.shape[1]
    width = wide // heads
    blocks = tokens // SPAN
    rows = tokens // n_tp
    n_z = n_tp // 2
    model = weight.shape[1]
    vm = pltpu.VMEM
    dma = pltpu.SemaphoreType.DMA
    return pl.pallas_call(
        functools.partial(mixer_kernel, (n_sp, n_tp, heads, capacity)),
        out_shape=[
            jax.ShapeDtypeStruct((rows, model), F32),
            jax.ShapeDtypeStruct((n_tp, 2 * experts, 2 * rows), F32),
        ],
        in_specs=[pl.BlockSpec(memory_space=vm)] * 10,
        out_specs=[pl.BlockSpec(memory_space=vm)] * 2,
        scratch_shapes=[
            vm((tokens, wide), F32),
            vm((tokens, wide), F32),
            vm((2, tokens, wide), F32),
            vm((2, blocks, 2 * width, wide), F32),
            vm((2, blocks, 2 * width, wide), F32),
            vm((2, 2 * width, wide), BF16),
            vm((n_sp, 2 * width, wide), BF16),
            vm((tokens, wide), BF16),
            vm((n_z, 2 * rows, model), BF16),
            vm((n_z, rows, model), BF16),
            vm((n_z, rows, model), BF16),
            vm((2 * n_z, rows, model), BF16),
            vm((n_tp, 2 * experts, 2 * rows), F32),
            dma((n_tp,)),
            dma((n_tp,)),
            dma((n_sp,)),
            dma((n_sp,)),
            dma((n_z,)),
            dma((n_z,)),
            dma((n_z,)),
            dma((2 * n_z,)),
        ],
        compiler_params=pltpu.CompilerParams(
            collective_id=0, has_side_effects=True, vmem_limit_bytes=56 * 1024 * 1024
        ),
        cost_estimate=pl.CostEstimate(flops=10**10, bytes_accessed=10**7, transcendentals=0),
    )(receptance, keys, values, erase, decay, spike.T, gain, weight, routes.T, routing.T)


def expert_kernel(
    geometry,
    input_ref, projected_ref, gain_ref, meta_ref, gate_hbm, up_hbm, down_hbm,
    shared_gate_hbm, shared_up_hbm, shared_down_hbm, out_ref,
    gate, up, down, shared_gate, shared_up, shared_down,
    residual, table, own, xg, sel_out, sel_in, y_buf, y_sib, sh_buf, sh_sib,
    q_out, q_in, t_out, t_in, fin, fin_sib,
    w_sem, own_sem, z_send, z_recv, xr_send, xr_recv, sel_send, sel_recv, sr_send, sr_recv,
    y_send, y_recv, sh_send, sh_recv, q_send, q_recv, t_send, t_recv, fin_sem,
):
    n_sp, n_tp, capacity = geometry
    n_z = n_tp // 2
    rows, model = input_ref.shape
    half = model // 2
    pair = 2 * rows
    slots = 2 * capacity
    local = gate_hbm.shape[0]
    experts = meta_ref.shape[1] // 2
    hidden = gate_hbm.shape[2]
    sp, tp = lax.axis_index("sp"), lax.axis_index("tp")
    z, core = tp // 2, lax.rem(tp, 2)
    other = 1 - core
    sibling = (sp, z * 2 + other)

    barrier = pltpu.get_barrier_semaphore()
    for d in range(1, n_sp):
        pl.semaphore_signal(barrier, inc=1, device_id=(lax.rem(sp + d, n_sp), tp), device_id_type=MESH)
    for d in range(1, n_z):
        pl.semaphore_signal(
            barrier, inc=1, device_id=(sp, lax.rem(z + d, n_z) * 2 + core), device_id_type=MESH
        )
    pl.semaphore_signal(barrier, inc=1, device_id=sibling, device_id_type=MESH)

    loads = [
        pltpu.make_async_copy(source, target, w_sem.at[i])
        for i, (source, target) in enumerate(
            [
                (gate_hbm, gate), (up_hbm, up), (down_hbm, down), (shared_gate_hbm, shared_gate),
                (shared_up_hbm, shared_up), (shared_down_hbm, shared_down),
            ]
        )
    ]
    for load in loads:
        load.start()

    def remote(source, target, send, recv, device):
        return pltpu.make_async_remote_copy(
            src_ref=source, dst_ref=target, send_sem=send, recv_sem=recv,
            device_id=device, device_id_type=MESH,
        )

    def rows_at(c):
        return pl.ds(pl.multiple_of(c * rows, rows), rows)

    total = input_ref[...].astype(F32) + projected_ref[...]
    residual[...] = total
    normed = total * lax.rsqrt(jnp.mean(total * total, axis=-1, keepdims=True) + RMS_EPS)
    normed = (normed * gain_ref[...].astype(F32).reshape(1, model)).astype(BF16)
    for h in range(2):
        own[h] = normed[:, h * half : (h + 1) * half]
        xg[z, h, rows_at(core), :] = normed[:, h * half : (h + 1) * half]
    for c in range(n_z):
        table[c] = meta_ref[2 * c] + meta_ref[2 * c + 1]
    pl.semaphore_wait(barrier, n_sp - 1 + n_z)

    own_copy = remote(own, xg.at[z, :, rows_at(core), :], own_sem.at[0], own_sem.at[1], sibling)
    own_copy.start()
    own_copy.wait_recv()

    def up_copy(c):
        there = xg.at[c, core]
        return remote(there, there, z_send.at[0, c], z_recv.at[c], (sp, lax.rem(z + 1, n_z) * 2 + core))

    def down_copy(c):
        there = xg.at[c, core]
        return remote(
            there, there, z_send.at[1, c], z_recv.at[c], (sp, lax.rem(z + n_z - 1, n_z) * 2 + core)
        )

    def along(c, act):
        @pl.when((c <= z) & (z < n_z - 1))
        def _():
            act(up_copy(c))

        @pl.when((c >= z) & (z > 0))
        def _():
            act(down_copy(c))

    near = near_order(n_z)
    along(z, lambda copy: copy.start())

    def relay_x(c):
        return remote(xg.at[c, core], xg.at[c, core], xr_send.at[c], xr_recv.at[c], sibling)

    def relay_x_in(c):
        return remote(xg.at[c, other], xg.at[c, other], xr_send.at[c], xr_recv.at[c], sibling)

    def sel_copy(c, g):
        return remote(
            sel_out.at[c, g], sel_in.at[c, core, :, sp], sel_send.at[c, g], sel_recv.at[c, sp],
            (g, tp),
        )

    def sel_arrival(c, g):
        return remote(
            sel_out.at[c, g], sel_in.at[c, core, :, g], sel_send.at[c, g], sel_recv.at[c, g], (g, tp)
        )

    def relay_sel(c, g):
        there = sel_in.at[c, core, :, g]
        return remote(there, there, sr_send.at[c, g], sr_recv.at[c, g], sibling)

    def relay_sel_in(c, g):
        there = sel_in.at[c, other, :, g]
        return remote(there, there, sr_send.at[c, g], sr_recv.at[c, g], sibling)

    slot_ids = (lax.broadcasted_iota(jnp.int32, (slots, pair), 0) + 1).astype(F32)

    def picks(c, g):
        return [(slot_ids == table[c, pl.ds(g * local + j, 1), :]).astype(F32) for j in range(local)]

    def select(c, g, h):
        chosen = jnp.concatenate(picks(c, g), axis=0).astype(BF16)
        return mul(chosen, xg[c, h]).astype(BF16).reshape(local, slots, half)

    def send_rows(c):
        for d in range(1, n_sp):
            g = lax.rem(sp + d, n_sp)
            sel_out[c, g] = select(c, g, core)
            sel_copy(c, g).start()

    send_rows(z)

    def take(k, carry):
        c = pick(near, z, k)
        up_copy(c).wait_recv()
        along(c, lambda copy: copy.start())
        relay_x(c).start()
        send_rows(c)
        return carry

    lax.fori_loop(0, n_z - 1, take, 0)
    for load in loads:
        load.wait()

    def feed(x, first, second):
        gate_value = mul(x[0], first[:half, :]) + mul(x[1], first[half:, :])
        up_value = mul(x[0], second[:half, :]) + mul(x[1], second[half:, :])
        return (jax.nn.silu(gate_value) * up_value).astype(BF16)

    def y_copy(c):
        return remote(y_buf.at[c, other], y_sib.at[c], y_send.at[c], y_recv.at[c], sibling)

    def sh_copy(c):
        return remote(sh_buf.at[c, other], sh_sib.at[c], sh_send.at[c], sh_recv.at[c], sibling)

    def q_copy(c, g):
        return remote(q_out.at[c, :, g], q_in.at[c, :, sp], q_send.at[c, g], q_recv.at[c, sp], (g, tp))

    def q_arrival(c, g):
        return remote(q_out.at[c, :, g], q_in.at[c, :, g], q_send.at[c, g], q_recv.at[c, g], (g, tp))

    def t_copy(c):
        return remote(t_out.at[c], t_in.at[z], t_send.at[c], t_recv.at[z], (sp, c * 2 + core))

    def t_arrival(c):
        return remote(t_out.at[c], t_in.at[c], t_send.at[c], t_recv.at[c], (sp, c * 2 + core))

    def combine(c):
        for d in range(1, n_sp):
            q_arrival(c, lax.rem(sp + d, n_sp)).wait_recv()
        result = sh_buf[c, core].astype(F32) + sh_sib[c].astype(F32)
        for j in range(local):
            weighted = []
            for g in range(n_sp):
                hot = slot_ids == table[c, g * local + j : g * local + j + 1, :]
                weight = table[c, experts + g * local + j : experts + g * local + j + 1, :]
                weighted.append(jnp.where(hot, weight, 0.0))
            high, low = halves(jnp.concatenate(weighted, axis=0))
            values = q_in[c, j].reshape(n_sp * slots, half)
            result = result + mul(high, values, TN) + mul(low, values, TN)
        return result

    def pass_on(c):
        t_out[c] = combine(c).astype(BF16)
        t_copy(c).start()

    out = out_order(n_z)

    def step(k, carry):
        c = pick(out, z, k)

        for d in range(1, n_sp):
            g = lax.rem(sp + n_sp - d, n_sp)
            sel_arrival(c, g).wait_recv()
            relay_sel(c, g).start()

        @pl.when(k < n_z - 1)
        def _():
            relay_x_in(c).wait_recv()

        for h in range(2):
            sel_in[c, h, :, sp] = select(c, sp, h)
        hidden_rows = feed([xg[c, 0], xg[c, 1]], shared_gate, shared_up)
        for h in range(2):
            sh_buf[c, h] = mul(hidden_rows, shared_down[:, h * half : (h + 1) * half]).astype(BF16)
        sh_copy(c).start()
        for d in range(1, n_sp):
            relay_sel_in(c, lax.rem(sp + n_sp - d, n_sp)).wait_recv()
        for j in range(local):
            x = [sel_in[c, h, j].reshape(n_sp * slots, half) for h in range(2)]
            hidden_rows = feed(x, gate.at[j], up.at[j])
            for h in range(2):
                y = mul(hidden_rows, down[j, :, h * half : (h + 1) * half]).astype(BF16)
                y_buf[c, h, j] = y.reshape(n_sp, slots, half)
        y_copy(c).start()

        @pl.when(k > 1)
        def _():
            pass_on(pick(out, z, k - 2))

        y_copy(c).wait_recv()
        sh_copy(c).wait_recv()
        q_out[c] = (y_buf[c, core].astype(F32) + y_sib[c].astype(F32)).astype(BF16)
        q_in[c, :, sp] = q_out[c, :, sp]
        for d in range(1, n_sp):
            q_copy(c, lax.rem(sp + d, n_sp)).start()
        return carry

    lax.fori_loop(0, n_z, step, 0)
    pass_on(pick(out, z, n_z - 2))
    fin[...] = combine(z)
    for d in range(1, n_z):
        c = lax.rem(z + d, n_z)
        t_arrival(c).wait_recv()
        fin[...] += t_in[c].astype(F32)
    fin_copy = remote(fin.at[rows_at(other), :], fin_sib, fin_sem.at[0], fin_sem.at[1], sibling)
    fin_copy.start()

    def columns(c):
        return pl.ds(pl.multiple_of(c * half, half), half)

    mine = residual[:, columns(core)] + fin[rows_at(core), :]
    out_ref[:, columns(core)] = mine.astype(out_ref.dtype)
    fin_copy.wait_recv()
    theirs = residual[:, columns(other)] + fin_sib[...]
    out_ref[:, columns(other)] = theirs.astype(out_ref.dtype)
    fin_copy.wait_send()
    own_copy.wait_send()
    for c in range(n_z):
        y_copy(c).wait_send()
        sh_copy(c).wait_send()
        for d in range(1, n_sp):
            g = lax.rem(sp + d, n_sp)
            sel_copy(c, g).wait_send()
            relay_sel(c, g).wait_send()
            q_copy(c, g).wait_send()
    for d in range(1, n_z):
        c = lax.rem(z + d, n_z)
        along(c, lambda copy: copy.wait_send())
        relay_x(c).wait_send()
        t_copy(c).wait_send()
    along(z, lambda copy: copy.wait_send())


def expert_shapes(n_sp, n_tp, rows, model, local, hidden, experts, capacity):
    n_z, half, pair, slots = n_tp // 2, model // 2, 2 * rows, 2 * capacity
    return [
        ((local, model, hidden), BF16),
        ((local, model, hidden), BF16),
        ((local, hidden, model), BF16),
        ((model, hidden), BF16),
        ((model, hidden), BF16),
        ((hidden, model), BF16),
        ((rows, model), F32),
        ((n_z, 2 * experts, pair), F32),
        ((2, rows, half), BF16),
        ((n_z, 2, pair, half), BF16),
        ((n_z, n_sp, local, slots, half), BF16),
        ((n_z, 2, local, n_sp, slots, half), BF16),
        ((n_z, 2, local, n_sp, slots, half), BF16),
        ((n_z, local, n_sp, slots, half), BF16),
        ((n_z, 2, pair, half), BF16),
        ((n_z, pair, half), BF16),
        ((n_z, local, n_sp, slots, half), BF16),
        ((n_z, local, n_sp, slots, half), BF16),
        ((n_z, pair, half), BF16),
        ((n_z, pair, half), BF16),
        ((pair, half), F32),
        ((rows, half), F32),
    ]


def expert_layer(
    n_sp, n_tp, shapes, capacity, layer_input, projected, gain, meta, gate, up, down,
    shared_gate, shared_up, shared_down,
):
    n_z = n_tp // 2
    vm = pltpu.VMEM
    dma = pltpu.SemaphoreType.DMA
    inside, outside = pl.BlockSpec(memory_space=vm), pl.BlockSpec(memory_space=pl.ANY)
    one, two = dma((n_z,)), dma((n_z, n_sp))
    return pl.pallas_call(
        functools.partial(expert_kernel, (n_sp, n_tp, capacity)),
        out_shape=jax.ShapeDtypeStruct(layer_input.shape, BF16),
        in_specs=[inside] * 4 + [outside] * 6,
        out_specs=inside,
        scratch_shapes=[vm(shape, dtype) for shape, dtype in shapes]
        + [dma((6,)), dma((2,)), dma((2, n_z)), one, one, one, two, two, two, two]
        + [one, one, one, one, two, two, one, one, dma((2,))],
        compiler_params=pltpu.CompilerParams(
            collective_id=1, has_side_effects=True, vmem_limit_bytes=VMEM_LIMIT
        ),
        cost_estimate=pl.CostEstimate(flops=10**10, bytes_accessed=10**7, transcendentals=0),
    )(
        layer_input, projected, gain, meta, gate, up, down,
        shared_gate, shared_up, shared_down,
    )


highest = lax.Precision.HIGHEST


def body(
    layer_input,
    receptance,
    keys,
    values,
    erase_preact,
    decay_preact,
    decay_spike,
    head_norm_gain,
    output_weight,
    expert_norm_gain,
    routes,
    routing_weight,
    expert_gate_weight,
    expert_up_weight,
    expert_down_weight,
    shared_gate_weight,
    shared_up_weight,
    shared_down_weight,
):
    row_count, model_width = layer_input.shape
    top_count = routes.shape[1]
    expert_local = expert_gate_weight.shape[0]
    sp_count, tp_count = lax.axis_size("sp"), lax.axis_size("tp")
    expert_total = expert_local * sp_count
    capacity = max(2, (3 * row_count * top_count + 2 * expert_total - 1) // (2 * expert_total))
    slot_total = sp_count * capacity * expert_local
    projected, meta = mixer(
        sp_count, tp_count, receptance, keys, values, erase_preact, decay_preact, decay_spike,
        head_norm_gain, output_weight, routes, routing_weight, expert_total, capacity,
    )
    shapes = expert_shapes(
        sp_count, tp_count, row_count, model_width, expert_local, expert_gate_weight.shape[2],
        expert_total, capacity,
    )
    used = sum(math.prod(shape) * jnp.dtype(dtype).itemsize for shape, dtype in shapes)
    if used < VMEM_LIMIT * 7 // 8 and (2 * capacity) % 16 == 0:
        return expert_layer(
            sp_count, tp_count, shapes, capacity, layer_input, projected, expert_norm_gain, meta,
            expert_gate_weight, expert_up_weight, expert_down_weight,
            shared_gate_weight, shared_up_weight, shared_down_weight,
        )
    residual = layer_input.astype(jnp.float32) + projected
    normed = residual * lax.rsqrt(jnp.mean(residual * residual, axis=-1, keepdims=True) + RMS_EPS)
    normed = (normed * expert_norm_gain.astype(jnp.float32)).astype(jnp.bfloat16)
    everyone = lax.all_gather(normed, "tp", axis=0, tiled=True)
    entries = routes.reshape(-1)
    entry_count = entries.shape[0]
    expert_hot = (entries[:, None] == lax.broadcasted_iota(jnp.int32, (1, expert_total), 1)).astype(
        jnp.int32
    )
    rank_in = jnp.sum((jnp.cumsum(expert_hot, axis=0) - 1) * expert_hot, axis=1)
    slot_of = entries * capacity + rank_in
    slot_hot = (slot_of[:, None] == lax.broadcasted_iota(jnp.int32, (1, slot_total), 1)).astype(
        jnp.float32
    )
    owner_hot = (
        lax.broadcasted_iota(jnp.int32, (entry_count, 1), 0) // top_count
        == lax.broadcasted_iota(jnp.int32, (1, row_count), 1)
    ).astype(jnp.float32)
    placing = jnp.dot(slot_hot.T, owner_hot, precision=highest)
    weighting = jnp.dot(owner_hot.T, slot_hot * routing_weight.reshape(-1, 1), precision=highest)
    outgoing = jnp.dot(placing.astype(jnp.bfloat16), normed, preferred_element_type=jnp.float32)
    outgoing = outgoing.astype(jnp.bfloat16).reshape(sp_count, expert_local, capacity, model_width)
    arrived = lax.all_to_all(outgoing, "sp", split_axis=0, concat_axis=0, tiled=True)

    def gathered(rows):
        return lax.all_gather(rows, "tp", axis=0, tiled=True)

    def hidden_layer(rows, gate, up, down):
        gate_value = jnp.dot(rows, gate, preferred_element_type=jnp.float32)
        up_value = jnp.dot(rows, up, preferred_element_type=jnp.float32)
        hidden = (jax.nn.silu(gate_value) * up_value).astype(jnp.bfloat16)
        partial_rows = jnp.dot(hidden, down, preferred_element_type=jnp.float32)
        return lax.psum_scatter(
            partial_rows.astype(jnp.bfloat16), "tp", scatter_dimension=0, tiled=True
        )

    shared = hidden_layer(everyone, shared_gate_weight, shared_up_weight, shared_down_weight)
    routed_rows = []
    for j in range(expert_local):
        rows = gathered(arrived[:, j].reshape(sp_count * capacity, model_width))
        out = hidden_layer(
            rows, expert_gate_weight[j], expert_up_weight[j], expert_down_weight[j]
        )
        routed_rows.append(out.reshape(sp_count, 1, capacity, model_width))
    routed_rows = jnp.concatenate(routed_rows, axis=1)
    returned = lax.all_to_all(routed_rows, "sp", split_axis=0, concat_axis=0, tiled=True)
    routed = jnp.dot(
        weighting, returned.reshape(slot_total, model_width).astype(jnp.float32), precision=highest
    )
    return (residual + shared.astype(jnp.float32) + routed).astype(jnp.bfloat16)


def solution(mesh):
    return jax.shard_map(
        body,
        mesh=mesh,
        in_specs=(
            P(("sp", "tp"), None),
            P("sp", "tp"),
            P("sp", "tp"),
            P("sp", "tp"),
            P("sp", "tp"),
            P("sp", "tp"),
            P("sp", "tp"),
            P("tp"),
            P("tp", None),
            P(),
            P(("sp", "tp"), None),
            P(("sp", "tp"), None),
            P("sp", None, "tp"),
            P("sp", None, "tp"),
            P("sp", "tp", None),
            P(None, "tp"),
            P(None, "tp"),
            P("tp", None),
        ),
        out_specs=P(("sp", "tp"), None),
        check_vma=False,
    )
```

```python
import functools
import math
import jax
import jax.numpy as jnp
from jax import lax
from jax.experimental import pallas as pl
from jax.experimental.pallas import tpu as pltpu
from jax.sharding import PartitionSpec as P

SPAN = 64
TOGETHER = 4
VMEM_LIMIT = 67043328
GN_EPS = 0.00064
RMS_EPS = 1e-06
F32, BF16 = jnp.float32, jnp.bfloat16
MESH = pl.DeviceIdType.MESH
NN = (((1,), (0,)), ((), ()))
NT = (((1,), (1,)), ((), ()))
TN = (((0,), (0,)), ((), ()))


def mul(left, right, dims=NN):
    return lax.dot_general(left, right, dims, preferred_element_type=F32)


def halves(x):
    high = x.astype(BF16)
    return high, (x - high.astype(F32)).astype(BF16)


def thirds(x):
    first = x.astype(BF16)
    rest = x - first.astype(F32)
    second = rest.astype(BF16)
    return first, second, (rest - second.astype(F32)).astype(BF16)


def product(left, right_high, right_low, dims=NN):
    rows = left.shape[0]
    high, low = halves(left)
    both = mul(jnp.concatenate([high, low], axis=0), right_high, dims)
    out = both[:rows] + both[rows:]
    if right_low is not None:
        out = out + mul(high, right_low, dims)
    return out


def near_order(n_z):
    table = []
    for z in range(n_z):
        others = sorted((c for c in range(n_z) if c != z), key=lambda c: (abs(c - z), c))
        table.append(others + [z])
    return table


def out_order(n_z):
    return [line[1:-1] + line[:1] + line[-1:] for line in near_order(n_z)]


def far_order(n_z):
    table = []
    for z in range(n_z):
        others = sorted((c for c in range(n_z) if c != z), key=lambda c: (-abs(c - z), c))
        table.append(others + [z])
    return table


def pick(table, z, k):
    found = jnp.int32(0)
    for i, line in enumerate(table):
        for j, value in enumerate(line):
            found = found + value * ((z == i) & (k == j)).astype(jnp.int32)
    return found


def route_table(routes, weights, experts, capacity, core):
    top, rows = routes.shape
    lines = lax.broadcasted_iota(jnp.int32, (experts, rows), 0)
    hot = jnp.zeros((experts, rows), F32)
    weight = jnp.zeros((experts, rows), F32)
    for j in range(top):
        chosen = routes[j : j + 1, :] == lines
        hot = hot + chosen.astype(F32)
        weight = weight + jnp.where(chosen, weights[j : j + 1, :], 0.0)
    row = lax.broadcasted_iota(jnp.int32, (rows, rows), 0)
    col = lax.broadcasted_iota(jnp.int32, (rows, rows), 1)
    rank = mul(hot.astype(BF16), (row < col).astype(F32).astype(BF16))
    place = (rank + 1.0 + (core * capacity).astype(F32)) * hot
    own = lax.broadcasted_iota(jnp.int32, (rows, 2 * rows), 0) + core * rows
    shifted = (own == lax.broadcasted_iota(jnp.int32, (rows, 2 * rows), 1)).astype(F32).astype(BF16)
    placed = mul(place.astype(BF16), shifted)
    weighed = sum(mul(part, shifted) for part in thirds(weight))
    return jnp.concatenate([placed, weighed], axis=0)


def mixer_kernel(
    geometry,
    r_ref, k_ref, v_ref, e_ref, dp_ref, spike_ref, gain_ref, w_ref, routes_ref, rw_ref,
    out_ref, meta_ref,
    spike_s, local_s, readout_s, maps_s, prefix_s, send_maps, recv_maps,
    mixed_s, part_s, sib_s, summed_s, recv_s,
    meta_s, meta_send, meta_recv, map_send, map_recv, sib_send, sib_recv, z_send, z_recv,
):
    n_sp, n_tp, heads, capacity = geometry
    n_z = n_tp // 2
    tokens, wide = k_ref.shape
    width = wide // heads
    blocks = tokens // SPAN
    rows = tokens // n_tp
    sp, tp = lax.axis_index("sp"), lax.axis_index("tp")
    z, core = tp // 2, lax.rem(tp, 2)

    barrier = pltpu.get_barrier_semaphore()
    for d in range(1, n_sp):
        pl.semaphore_signal(barrier, inc=1, device_id=(lax.rem(sp + d, n_sp), tp), device_id_type=MESH)
    for d in range(1, n_tp):
        pl.semaphore_signal(barrier, inc=1, device_id=(sp, lax.rem(tp + d, n_tp)), device_id_type=MESH)

    def head_mask(shape, dtype):
        first = lax.broadcasted_iota(jnp.int32, shape, 0) // width
        second = lax.broadcasted_iota(jnp.int32, shape, 1) // width
        return (first == second).astype(F32).astype(dtype)

    square = head_mask((wide, wide), BF16)

    def spread(x):
        return jnp.concatenate([x] * heads, axis=0) * square

    def spread_pair(x):
        high, low = halves(x)
        return spread(high), spread(low)

    def gather_heads(x):
        total = x[:width]
        for h in range(1, heads):
            total = total + x[h * width : (h + 1) * width]
        return total

    def lane_of(shape):
        return lax.broadcasted_iota(jnp.int32, shape, 1)

    row_t = lax.broadcasted_iota(jnp.int32, (SPAN, wide), 0)
    col_s = lax.rem(lane_of((SPAN, wide)), SPAN)
    below = row_t > col_s
    above = row_t < col_s
    same = row_t == col_s
    tri = (
        lax.broadcasted_iota(jnp.int32, (SPAN, SPAN), 0)
        >= lax.broadcasted_iota(jnp.int32, (SPAN, SPAN), 1)
    ).astype(F32).astype(BF16)
    tri3 = jnp.concatenate([tri, tri, tri], axis=1)
    eye = same.astype(F32)

    def product_all(lefts, rights, dims=NN):
        pairs = [spread_pair(right) for right in rights]
        return [product(left, *pair, dims=dims) for left, pair in zip(lefts, pairs)]

    def each_group(i, carry):
        chains = []
        blocks_here = []
        for b in [i * TOGETHER + n for n in range(TOGETHER)]:
            here = pl.ds(pl.multiple_of(b * SPAN, SPAN), SPAN)
            keys = k_ref[here, :].astype(F32)
            square_high, square_low = halves(keys * keys)
            norm = mul(jnp.concatenate([square_high, square_low], axis=0), square)
            norm = norm[:SPAN] + norm[SPAN:]
            unit = keys * lax.rsqrt(norm + 1e-06)
            beta = unit * jax.nn.sigmoid(e_ref[here, :].astype(F32))
            decay = -0.6065306597126334 * jax.nn.sigmoid(dp_ref[here, :].astype(F32))
            decay = decay + spike_s[here, :]
            decay_1, decay_2, decay_3 = thirds(decay)
            cumulative = mul(tri3, jnp.concatenate([decay_1, decay_2, decay_3], axis=0))
            total = cumulative[SPAN - 1 : SPAN, :]
            middle = 0.5 * total
            e1 = jnp.exp(cumulative - middle)
            e2 = jnp.exp(cumulative - decay - middle)
            e3 = jnp.exp(middle - cumulative)
            e4 = jnp.exp(middle - cumulative + decay)
            em = jnp.exp(middle)
            et = jnp.exp(total)
            reads = r_ref[here, :].astype(F32)
            values = v_ref[here, :]
            value_wide = spread(values)
            blocks_here.append((b, here))
            for d in range(2):
                left_scale, before_scale, right_scale = (e1, e2, e3) if d == 0 else (e4, e3, e2)
                left = jnp.concatenate([unit * before_scale, reads * left_scale], axis=0)
                chains.append(
                    (d, b, here, left, beta * right_scale, keys * right_scale, em, et, values, value_wide)
                )
        lefts = [c[3] for c in chains]
        keeps = []
        for c in chains:
            strict = below if c[0] == 0 else above
            keeps.append(jnp.concatenate([strict, strict | same], axis=0))
        from_beta = product_all(lefts, [c[4] for c in chains], NT)
        from_beta = [jnp.where(keep, x, 0.0) for keep, x in zip(keeps, from_beta)]
        from_key = product_all(lefts, [c[5] for c in chains], NT)
        from_key = [jnp.where(keep, x, 0.0) for keep, x in zip(keeps, from_key)]
        key_part = [product(x, c[9], None) for x, c in zip(from_key, chains)]
        size, inverse = 1, None
        while size < SPAN:
            corner_mask = (row_t // (2 * size) == col_s // (2 * size)) & (row_t // size != col_s // size)
            corner = [jnp.where(corner_mask, x[:SPAN], 0.0) for x in from_beta]
            if size == 1:
                inverse = [eye - x for x in corner]
            else:
                steps = product_all(corner, inverse)
                steps = product_all(inverse, steps)
                inverse = [x - y for x, y in zip(inverse, steps)]
            size *= 2
        true_left = [c[3] * c[6] for c in chains]
        solved_w = product_all(inverse, [x[:SPAN] for x in true_left])
        solved_v = product_all(inverse, [-x[:SPAN] for x in key_part])
        read = [x[SPAN:] for x in from_beta]
        read_v = product_all(read, solved_v)
        read_w = product_all(read, solved_w)
        on_head = lax.broadcasted_iota(jnp.int32, (width, wide), 0) == lax.rem(
            lane_of((width, wide)), width
        )
        wide_mask = square.astype(F32)
        locals_now = []
        for n, (d, b, here, left, beta_right, key_right, em, et, values, value_wide) in enumerate(chains):
            locals_now.append(key_part[n][SPAN:] + read_v[n])
            readout_s[d, here, :] = true_left[n][SPAN:] - read_w[n]
            beta_high, beta_low = halves(beta_right * em)
            key_high, key_low = halves(key_right * em)
            w_high, w_low = halves(solved_w[n])
            v_high, v_low = halves(solved_v[n])
            beta_three = [beta_high, beta_low, beta_high]
            move = mul(
                jnp.concatenate([w_high, w_high, w_low], axis=0),
                jnp.concatenate(beta_three, axis=0),
                TN,
            )
            put = mul(
                jnp.concatenate([v_high, v_high, v_low, values, values], axis=0),
                jnp.concatenate(beta_three + [key_high, key_low], axis=0),
                TN,
            )
            move = gather_heads(move * wide_mask)
            maps_s[d, b, :width, :] = jnp.where(on_head, et, 0.0) - move
            maps_s[d, b, width:, :] = gather_heads(put * wide_mask)
        for n, (b, here) in enumerate(blocks_here):
            local_s[here, :] = locals_now[2 * n] + locals_now[2 * n + 1]
        return carry

    head_row = lax.broadcasted_iota(jnp.int32, (heads, wide), 0)
    head_hot = (head_row == lane_of((heads, wide)) // width).astype(F32).astype(BF16)
    spike_s[...] = sum(mul(part, head_hot, TN) for part in thirds(spike_ref[...]))

    lax.fori_loop(0, blocks // TOGETHER, each_group, 0)

    first = (
        lax.broadcasted_iota(jnp.int32, (2 * width, wide), 0)
        == lax.rem(lane_of((2 * width, wide)), width)
    ).astype(F32)
    no_rows = jnp.zeros((width, wide), F32)

    def compose(i, carry):
        new = []
        for d in range(2):
            b = i if d == 0 else blocks - 1 - i
            prefix_s[d, b] = carry[d]
            moved = product(carry[d], *spread_pair(maps_s[d, b, :width, :]))
            new.append(moved + jnp.concatenate([no_rows, maps_s[d, b, width:, :]], axis=0))
        return tuple(new)

    whole = lax.fori_loop(0, blocks, compose, (first, first))
    for d in range(2):
        send_maps[d] = whole[d].astype(BF16)
    pl.semaphore_wait(barrier, n_sp - 1 + n_tp - 1)

    copies = []
    for d in range(1, n_sp):
        target = lax.rem(sp + d, n_sp)
        copy = pltpu.make_async_remote_copy(
            src_ref=send_maps.at[(target < sp).astype(jnp.int32)],
            dst_ref=recv_maps.at[sp],
            send_sem=map_send.at[d],
            recv_sem=map_recv.at[sp],
            device_id=(target, tp),
            device_id_type=MESH,
        )
        copy.start()
        copies.append(copy)

    experts = meta_ref.shape[1] // 2
    meta_s[tp] = route_table(routes_ref[...], rw_ref[...], experts, capacity, core)

    def meta_copy(d):
        return pltpu.make_async_remote_copy(
            src_ref=meta_s.at[tp],
            dst_ref=meta_s.at[tp],
            send_sem=meta_send.at[d],
            recv_sem=meta_recv.at[tp],
            device_id=(sp, lax.rem(tp + d, n_tp)),
            device_id_type=MESH,
        )

    for d in range(1, n_tp):
        meta_copy(d).start()

    for d in range(1, n_sp):
        source = lax.rem(sp + d, n_sp)
        pltpu.make_async_remote_copy(
            src_ref=send_maps.at[0],
            dst_ref=recv_maps.at[source],
            send_sem=map_send.at[d],
            recv_sem=map_recv.at[source],
            device_id=(source, tp),
            device_id_type=MESH,
        ).wait_recv()
    for copy in copies:
        copy.wait_send()
    recv_maps[sp] = jnp.zeros((2 * width, wide), BF16)

    def enter(i, carry):
        new = []
        for d in range(2):
            k = i if d == 0 else n_sp - 1 - i
            reached = (k < sp) if d == 0 else (k > sp)
            part = recv_maps[k]
            moved = product(carry[d], spread(part[:width]), None) + part[width:].astype(F32)
            new.append(jnp.where(reached, moved, carry[d]))
        return tuple(new)

    entry = lax.fori_loop(0, n_sp, enter, (no_rows, no_rows))

    gain = gain_ref[...].astype(F32).reshape(1, wide)

    def finish(b, carry):
        here = pl.ds(pl.multiple_of(b * SPAN, SPAN), SPAN)
        mix = local_s[here, :]
        for d in range(2):
            start = product(entry[d], *spread_pair(prefix_s[d, b, :width, :]))
            start = start + prefix_s[d, b, width:, :]
            mix = mix + product(readout_s[d, here, :], *spread_pair(start), dims=NT)
        mean = product(mix, square, None) * (1.0 / width)
        mix = mix - mean
        spread_of = product(mix * mix, square, None) * (1.0 / width)
        mixed = mix * lax.rsqrt(spread_of + GN_EPS) * gain
        mixed_s[here, :] = mixed.astype(BF16)
        return carry

    sibling = (sp, z * 2 + 1 - core)

    def sib_copy(c):
        return pltpu.make_async_remote_copy(
            src_ref=part_s.at[c, pl.ds(pl.multiple_of((1 - core) * rows, rows), rows), :],
            dst_ref=sib_s.at[c],
            send_sem=sib_send.at[c],
            recv_sem=sib_recv.at[c],
            device_id=sibling,
            device_id_type=MESH,
        )

    low_end = ((z == 0) & (n_z > 2)).astype(jnp.int32)
    high_end = ((z == n_z - 1) & (n_z > 2)).astype(jnp.int32)
    at_end = low_end + high_end
    inner = low_end + high_end * (n_z - 2)

    def z_copy(c):
        through = at_end * (c != inner).astype(jnp.int32)
        slot = through * (n_z + c) + (1 - through) * z
        target = at_end * inner + (1 - at_end) * c
        return pltpu.make_async_remote_copy(
            src_ref=summed_s.at[c],
            dst_ref=recv_s.at[slot],
            send_sem=z_send.at[c],
            recv_sem=z_recv.at[slot],
            device_id=(sp, target * 2 + core),
            device_id_type=MESH,
        )

    def arrival(slot):
        return pltpu.make_async_remote_copy(
            src_ref=summed_s.at[0],
            dst_ref=recv_s.at[slot],
            send_sem=z_send.at[0],
            recv_sem=z_recv.at[slot],
            device_id=sibling,
            device_id_type=MESH,
        )

    def joins(c):
        return (n_z > 2) & (((z == 1) & (c > 1)) | ((z == n_z - 2) & (c < n_z - 2)))

    far = far_order(n_z)

    def chip_at(i):
        return pick(far, z, i)

    def pass_on(i):
        c = chip_at(i)
        sib_copy(c).wait_recv()
        mine = part_s[c, pl.ds(pl.multiple_of(core * rows, rows), rows), :].astype(F32)
        mine = mine + sib_s[c].astype(F32)
        summed_s[c] = mine.astype(BF16)

        @pl.when((c != z) & jnp.logical_not(joins(c)))
        def _():
            z_copy(c).start()

    def project(i, carry):
        c = chip_at(i)
        there = pl.ds(pl.multiple_of(c * (2 * rows), 2 * rows), 2 * rows)
        first_block = c * (2 * rows // SPAN)
        for n in range(2 * rows // SPAN):
            finish(first_block + n, 0)
        part_s[c] = mul(mixed_s[there, :], w_ref[...]).astype(BF16)
        sib_copy(c).start()
        pass_on(i)
        return carry

    lax.fori_loop(0, n_z, project, 0)
    for i in range(n_z - 1):
        c = chip_at(i)

        @pl.when(joins(c))
        def _():
            arrival(n_z + c).wait_recv()
            summed_s[c] = (summed_s[c].astype(F32) + recv_s[n_z + c].astype(F32)).astype(BF16)
            z_copy(c).start()

    out_ref[...] = summed_s[z].astype(F32)
    for source in range(n_z):
        direct = z != source
        if n_z > 2 and source == 0:
            direct = z == 1
        if n_z > 2 and source == n_z - 1:
            direct = z == n_z - 2

        @pl.when(direct)
        def _():
            arrival(source).wait_recv()
            out_ref[...] += recv_s[source].astype(F32)

    for d in range(1, n_z):
        z_copy(lax.rem(z + d, n_z)).wait_send()
    for c in range(n_z):
        sib_copy(c).wait_send()
    for d in range(1, n_tp):
        source = lax.rem(tp + d, n_tp)
        pltpu.make_async_remote_copy(
            src_ref=meta_s.at[tp],
            dst_ref=meta_s.at[source],
            send_sem=meta_send.at[d],
            recv_sem=meta_recv.at[source],
            device_id=(sp, source),
            device_id_type=MESH,
        ).wait_recv()
        meta_copy(d).wait_send()
    meta_ref[...] = meta_s[...]


def mixer(n_sp, n_tp, receptance, keys, values, erase, decay, spike, gain, weight, routes, routing, experts, capacity):
    tokens, wide = keys.shape
    heads = spike.shape[1]
    width = wide // heads
    blocks = tokens // SPAN
    rows = tokens // n_tp
    n_z = n_tp // 2
    model = weight.shape[1]
    vm = pltpu.VMEM
    dma = pltpu.SemaphoreType.DMA
    return pl.pallas_call(
        functools.partial(mixer_kernel, (n_sp, n_tp, heads, capacity)),
        out_shape=[
            jax.ShapeDtypeStruct((rows, model), F32),
            jax.ShapeDtypeStruct((n_tp, 2 * experts, 2 * rows), F32),
        ],
        in_specs=[pl.BlockSpec(memory_space=vm)] * 10,
        out_specs=[pl.BlockSpec(memory_space=vm)] * 2,
        scratch_shapes=[
            vm((tokens, wide), F32),
            vm((tokens, wide), F32),
            vm((2, tokens, wide), F32),
            vm((2, blocks, 2 * width, wide), F32),
            vm((2, blocks, 2 * width, wide), F32),
            vm((2, 2 * width, wide), BF16),
            vm((n_sp, 2 * width, wide), BF16),
            vm((tokens, wide), BF16),
            vm((n_z, 2 * rows, model), BF16),
            vm((n_z, rows, model), BF16),
            vm((n_z, rows, model), BF16),
            vm((2 * n_z, rows, model), BF16),
            vm((n_tp, 2 * experts, 2 * rows), F32),
            dma((n_tp,)),
            dma((n_tp,)),
            dma((n_sp,)),
            dma((n_sp,)),
            dma((n_z,)),
            dma((n_z,)),
            dma((n_z,)),
            dma((2 * n_z,)),
        ],
        compiler_params=pltpu.CompilerParams(
            collective_id=0, has_side_effects=True, vmem_limit_bytes=56 * 1024 * 1024
        ),
        cost_estimate=pl.CostEstimate(flops=10**10, bytes_accessed=10**7, transcendentals=0),
    )(receptance, keys, values, erase, decay, spike.T, gain, weight, routes.T, routing.T)


def expert_kernel(
    geometry,
    input_ref, projected_ref, gain_ref, meta_ref, gate_hbm, up_hbm, down_hbm,
    shared_gate_hbm, shared_up_hbm, shared_down_hbm, out_ref,
    gate, up, down, shared_gate, shared_up, shared_down,
    residual, table, own, xg, sel_out, sel_in, y_buf, y_sib, sh_buf, sh_sib,
    q_out, q_in, t_out, t_in, fin, fin_sib,
    w_sem, own_sem, z_send, z_recv, xr_send, xr_recv, sel_send, sel_recv, sr_send, sr_recv,
    y_send, y_recv, sh_send, sh_recv, q_send, q_recv, t_send, t_recv, fin_sem,
):
    n_sp, n_tp, capacity = geometry
    n_z = n_tp // 2
    rows, model = input_ref.shape
    half = model // 2
    pair = 2 * rows
    slots = 2 * capacity
    local = gate_hbm.shape[0]
    experts = meta_ref.shape[1] // 2
    hidden = gate_hbm.shape[2]
    sp, tp = lax.axis_index("sp"), lax.axis_index("tp")
    z, core = tp // 2, lax.rem(tp, 2)
    other = 1 - core
    sibling = (sp, z * 2 + other)

    barrier = pltpu.get_barrier_semaphore()
    for d in range(1, n_sp):
        pl.semaphore_signal(barrier, inc=1, device_id=(lax.rem(sp + d, n_sp), tp), device_id_type=MESH)
    for d in range(1, n_z):
        pl.semaphore_signal(
            barrier, inc=1, device_id=(sp, lax.rem(z + d, n_z) * 2 + core), device_id_type=MESH
        )
    pl.semaphore_signal(barrier, inc=1, device_id=sibling, device_id_type=MESH)

    loads = [
        pltpu.make_async_copy(source, target, w_sem.at[i])
        for i, (source, target) in enumerate(
            [
                (gate_hbm, gate), (up_hbm, up), (down_hbm, down), (shared_gate_hbm, shared_gate),
                (shared_up_hbm, shared_up), (shared_down_hbm, shared_down),
            ]
        )
    ]
    for load in loads:
        load.start()

    def remote(source, target, send, recv, device):
        return pltpu.make_async_remote_copy(
            src_ref=source, dst_ref=target, send_sem=send, recv_sem=recv,
            device_id=device, device_id_type=MESH,
        )

    def rows_at(c):
        return pl.ds(pl.multiple_of(c * rows, rows), rows)

    total = input_ref[...].astype(F32) + projected_ref[...]
    residual[...] = total
    normed = total * lax.rsqrt(jnp.mean(total * total, axis=-1, keepdims=True) + RMS_EPS)
    normed = (normed * gain_ref[...].astype(F32).reshape(1, model)).astype(BF16)
    for h in range(2):
        own[h] = normed[:, h * half : (h + 1) * half]
        xg[z, h, rows_at(core), :] = normed[:, h * half : (h + 1) * half]
    for c in range(n_z):
        table[c] = meta_ref[2 * c] + meta_ref[2 * c + 1]
    pl.semaphore_wait(barrier, n_sp - 1 + n_z)

    own_copy = remote(own, xg.at[z, :, rows_at(core), :], own_sem.at[0], own_sem.at[1], sibling)
    own_copy.start()
    own_copy.wait_recv()

    def up_copy(c):
        there = xg.at[c, core]
        return remote(there, there, z_send.at[0, c], z_recv.at[c], (sp, lax.rem(z + 1, n_z) * 2 + core))

    def down_copy(c):
        there = xg.at[c, core]
        return remote(
            there, there, z_send.at[1, c], z_recv.at[c], (sp, lax.rem(z + n_z - 1, n_z) * 2 + core)
        )

    def along(c, act):
        @pl.when((c <= z) & (z < n_z - 1))
        def _():
            act(up_copy(c))

        @pl.when((c >= z) & (z > 0))
        def _():
            act(down_copy(c))

    near = near_order(n_z)
    along(z, lambda copy: copy.start())

    def relay_x(c):
        return remote(xg.at[c, core], xg.at[c, core], xr_send.at[c], xr_recv.at[c], sibling)

    def relay_x_in(c):
        return remote(xg.at[c, other], xg.at[c, other], xr_send.at[c], xr_recv.at[c], sibling)

    def sel_copy(c, g):
        return remote(
            sel_out.at[c, g], sel_in.at[c, core, :, sp], sel_send.at[c, g], sel_recv.at[c, sp],
            (g, tp),
        )

    def sel_arrival(c, g):
        return remote(
            sel_out.at[c, g], sel_in.at[c, core, :, g], sel_send.at[c, g], sel_recv.at[c, g], (g, tp)
        )

    def relay_sel(c, g):
        there = sel_in.at[c, core, :, g]
        return remote(there, there, sr_send.at[c, g], sr_recv.at[c, g], sibling)

    def relay_sel_in(c, g):
        there = sel_in.at[c, other, :, g]
        return remote(there, there, sr_send.at[c, g], sr_recv.at[c, g], sibling)

    slot_ids = (lax.broadcasted_iota(jnp.int32, (slots, pair), 0) + 1).astype(F32)

    def picks(c, g):
        return [(slot_ids == table[c, pl.ds(g * local + j, 1), :]).astype(F32) for j in range(local)]

    def select(c, g, h):
        chosen = jnp.concatenate(picks(c, g), axis=0).astype(BF16)
        return mul(chosen, xg[c, h]).astype(BF16).reshape(local, slots, half)

    def send_rows(c):
        for d in range(1, n_sp):
            g = lax.rem(sp + d, n_sp)
            sel_out[c, g] = select(c, g, core)
            sel_copy(c, g).start()

    send_rows(z)

    def take(k, carry):
        c = pick(near, z, k)
        up_copy(c).wait_recv()
        along(c, lambda copy: copy.start())
        relay_x(c).start()
        send_rows(c)
        return carry

    lax.fori_loop(0, n_z - 1, take, 0)
    for load in loads:
        load.wait()

    def feed(x, first, second):
        gate_value = mul(x[0], first[:half, :]) + mul(x[1], first[half:, :])
        up_value = mul(x[0], second[:half, :]) + mul(x[1], second[half:, :])
        return (jax.nn.silu(gate_value) * up_value).astype(BF16)

    def y_copy(c):
        return remote(y_buf.at[c, other], y_sib.at[c], y_send.at[c], y_recv.at[c], sibling)

    def sh_copy(c):
        return remote(sh_buf.at[c, other], sh_sib.at[c], sh_send.at[c], sh_recv.at[c], sibling)

    def q_copy(c, g):
        return remote(q_out.at[c, :, g], q_in.at[c, :, sp], q_send.at[c, g], q_recv.at[c, sp], (g, tp))

    def q_arrival(c, g):
        return remote(q_out.at[c, :, g], q_in.at[c, :, g], q_send.at[c, g], q_recv.at[c, g], (g, tp))

    def t_copy(c):
        return remote(t_out.at[c], t_in.at[z], t_send.at[c], t_recv.at[z], (sp, c * 2 + core))

    def t_arrival(c):
        return remote(t_out.at[c], t_in.at[c], t_send.at[c], t_recv.at[c], (sp, c * 2 + core))

    def combine(c):
        for d in range(1, n_sp):
            q_arrival(c, lax.rem(sp + d, n_sp)).wait_recv()
        result = sh_buf[c, core].astype(F32) + sh_sib[c].astype(F32)
        for j in range(local):
            weighted = []
            for g in range(n_sp):
                hot = slot_ids == table[c, g * local + j : g * local + j + 1, :]
                weight = table[c, experts + g * local + j : experts + g * local + j + 1, :]
                weighted.append(jnp.where(hot, weight, 0.0))
            high, low = halves(jnp.concatenate(weighted, axis=0))
            values = q_in[c, j].reshape(n_sp * slots, half)
            result = result + mul(high, values, TN) + mul(low, values, TN)
        return result

    def pass_on(c):
        t_out[c] = combine(c).astype(BF16)
        t_copy(c).start()

    out = out_order(n_z)

    def step(k, carry):
        c = pick(out, z, k)

        for d in range(1, n_sp):
            g = lax.rem(sp + n_sp - d, n_sp)
            sel_arrival(c, g).wait_recv()
            relay_sel(c, g).start()

        @pl.when(k < n_z - 1)
        def _():
            relay_x_in(c).wait_recv()

        for h in range(2):
            sel_in[c, h, :, sp] = select(c, sp, h)
        hidden_rows = feed([xg[c, 0], xg[c, 1]], shared_gate, shared_up)
        for h in range(2):
            sh_buf[c, h] = mul(hidden_rows, shared_down[:, h * half : (h + 1) * half]).astype(BF16)
        sh_copy(c).start()
        for d in range(1, n_sp):
            relay_sel_in(c, lax.rem(sp + n_sp - d, n_sp)).wait_recv()
        for j in range(local):
            x = [sel_in[c, h, j].reshape(n_sp * slots, half) for h in range(2)]
            hidden_rows = feed(x, gate.at[j], up.at[j])
            for h in range(2):
                y = mul(hidden_rows, down[j, :, h * half : (h + 1) * half]).astype(BF16)
                y_buf[c, h, j] = y.reshape(n_sp, slots, half)
        y_copy(c).start()

        @pl.when(k > 1)
        def _():
            pass_on(pick(out, z, k - 2))

        y_copy(c).wait_recv()
        sh_copy(c).wait_recv()
        q_out[c] = (y_buf[c, core].astype(F32) + y_sib[c].astype(F32)).astype(BF16)
        q_in[c, :, sp] = q_out[c, :, sp]
        for d in range(1, n_sp):
            q_copy(c, lax.rem(sp + d, n_sp)).start()
        return carry

    lax.fori_loop(0, n_z, step, 0)
    pass_on(pick(out, z, n_z - 2))
    fin[...] = combine(z)
    for d in range(1, n_z):
        c = lax.rem(z + d, n_z)
        t_arrival(c).wait_recv()
        fin[...] += t_in[c].astype(F32)
    fin_copy = remote(fin.at[rows_at(other), :], fin_sib, fin_sem.at[0], fin_sem.at[1], sibling)
    fin_copy.start()

    def columns(c):
        return pl.ds(pl.multiple_of(c * half, half), half)

    mine = residual[:, columns(core)] + fin[rows_at(core), :]
    out_ref[:, columns(core)] = mine.astype(out_ref.dtype)
    fin_copy.wait_recv()
    theirs = residual[:, columns(other)] + fin_sib[...]
    out_ref[:, columns(other)] = theirs.astype(out_ref.dtype)
    fin_copy.wait_send()
    own_copy.wait_send()
    for c in range(n_z):
        y_copy(c).wait_send()
        sh_copy(c).wait_send()
        for d in range(1, n_sp):
            g = lax.rem(sp + d, n_sp)
            sel_copy(c, g).wait_send()
            relay_sel(c, g).wait_send()
            q_copy(c, g).wait_send()
    for d in range(1, n_z):
        c = lax.rem(z + d, n_z)
        along(c, lambda copy: copy.wait_send())
        relay_x(c).wait_send()
        t_copy(c).wait_send()
    along(z, lambda copy: copy.wait_send())


def expert_shapes(n_sp, n_tp, rows, model, local, hidden, experts, capacity):
    n_z, half, pair, slots = n_tp // 2, model // 2, 2 * rows, 2 * capacity
    return [
        ((local, model, hidden), BF16),
        ((local, model, hidden), BF16),
        ((local, hidden, model), BF16),
        ((model, hidden), BF16),
        ((model, hidden), BF16),
        ((hidden, model), BF16),
        ((rows, model), F32),
        ((n_z, 2 * experts, pair), F32),
        ((2, rows, half), BF16),
        ((n_z, 2, pair, half), BF16),
        ((n_z, n_sp, local, slots, half), BF16),
        ((n_z, 2, local, n_sp, slots, half), BF16),
        ((n_z, 2, local, n_sp, slots, half), BF16),
        ((n_z, local, n_sp, slots, half), BF16),
        ((n_z, 2, pair, half), BF16),
        ((n_z, pair, half), BF16),
        ((n_z, local, n_sp, slots, half), BF16),
        ((n_z, local, n_sp, slots, half), BF16),
        ((n_z, pair, half), BF16),
        ((n_z, pair, half), BF16),
        ((pair, half), F32),
        ((rows, half), F32),
    ]


def expert_layer(
    n_sp, n_tp, shapes, capacity, layer_input, projected, gain, meta, gate, up, down,
    shared_gate, shared_up, shared_down,
):
    n_z = n_tp // 2
    vm = pltpu.VMEM
    dma = pltpu.SemaphoreType.DMA
    inside, outside = pl.BlockSpec(memory_space=vm), pl.BlockSpec(memory_space=pl.ANY)
    one, two = dma((n_z,)), dma((n_z, n_sp))
    return pl.pallas_call(
        functools.partial(expert_kernel, (n_sp, n_tp, capacity)),
        out_shape=jax.ShapeDtypeStruct(layer_input.shape, BF16),
        in_specs=[inside] * 4 + [outside] * 6,
        out_specs=inside,
        scratch_shapes=[vm(shape, dtype) for shape, dtype in shapes]
        + [dma((6,)), dma((2,)), dma((2, n_z)), one, one, one, two, two, two, two]
        + [one, one, one, one, two, two, one, one, dma((2,))],
        compiler_params=pltpu.CompilerParams(
            collective_id=1, has_side_effects=True, vmem_limit_bytes=VMEM_LIMIT
        ),
        cost_estimate=pl.CostEstimate(flops=10**10, bytes_accessed=10**7, transcendentals=0),
    )(
        layer_input, projected, gain, meta, gate, up, down,
        shared_gate, shared_up, shared_down,
    )


highest = lax.Precision.HIGHEST


def body(
    layer_input,
    receptance,
    keys,
    values,
    erase_preact,
    decay_preact,
    decay_spike,
    head_norm_gain,
    output_weight,
    expert_norm_gain,
    routes,
    routing_weight,
    expert_gate_weight,
    expert_up_weight,
    expert_down_weight,
    shared_gate_weight,
    shared_up_weight,
    shared_down_weight,
):
    row_count, model_width = layer_input.shape
    top_count = routes.shape[1]
    expert_local = expert_gate_weight.shape[0]
    sp_count, tp_count = lax.axis_size("sp"), lax.axis_size("tp")
    expert_total = expert_local * sp_count
    capacity = max(2, (3 * row_count * top_count + 2 * expert_total - 1) // (2 * expert_total))
    slot_total = sp_count * capacity * expert_local
    projected, meta = mixer(
        sp_count, tp_count, receptance, keys, values, erase_preact, decay_preact, decay_spike,
        head_norm_gain, output_weight, routes, routing_weight, expert_total, capacity,
    )
    shapes = expert_shapes(
        sp_count, tp_count, row_count, model_width, expert_local, expert_gate_weight.shape[2],
        expert_total, capacity,
    )
    used = sum(math.prod(shape) * jnp.dtype(dtype).itemsize for shape, dtype in shapes)
    if used < VMEM_LIMIT * 7 // 8 and (2 * capacity) % 16 == 0:
        return expert_layer(
            sp_count, tp_count, shapes, capacity, layer_input, projected, expert_norm_gain, meta,
            expert_gate_weight, expert_up_weight, expert_down_weight,
            shared_gate_weight, shared_up_weight, shared_down_weight,
        )
    residual = layer_input.astype(jnp.float32) + projected
    normed = residual * lax.rsqrt(jnp.mean(residual * residual, axis=-1, keepdims=True) + RMS_EPS)
    normed = (normed * expert_norm_gain.astype(jnp.float32)).astype(jnp.bfloat16)
    everyone = lax.all_gather(normed, "tp", axis=0, tiled=True)
    entries = routes.reshape(-1)
    entry_count = entries.shape[0]
    expert_hot = (entries[:, None] == lax.broadcasted_iota(jnp.int32, (1, expert_total), 1)).astype(
        jnp.int32
    )
    rank_in = jnp.sum((jnp.cumsum(expert_hot, axis=0) - 1) * expert_hot, axis=1)
    slot_of = entries * capacity + rank_in
    slot_hot = (slot_of[:, None] == lax.broadcasted_iota(jnp.int32, (1, slot_total), 1)).astype(
        jnp.float32
    )
    owner_hot = (
        lax.broadcasted_iota(jnp.int32, (entry_count, 1), 0) // top_count
        == lax.broadcasted_iota(jnp.int32, (1, row_count), 1)
    ).astype(jnp.float32)
    placing = jnp.dot(slot_hot.T, owner_hot, precision=highest)
    weighting = jnp.dot(owner_hot.T, slot_hot * routing_weight.reshape(-1, 1), precision=highest)
    outgoing = jnp.dot(placing.astype(jnp.bfloat16), normed, preferred_element_type=jnp.float32)
    outgoing = outgoing.astype(jnp.bfloat16).reshape(sp_count, expert_local, capacity, model_width)
    arrived = lax.all_to_all(outgoing, "sp", split_axis=0, concat_axis=0, tiled=True)

    def gathered(rows):
        return lax.all_gather(rows, "tp", axis=0, tiled=True)

    def hidden_layer(rows, gate, up, down):
        gate_value = jnp.dot(rows, gate, preferred_element_type=jnp.float32)
        up_value = jnp.dot(rows, up, preferred_element_type=jnp.float32)
        hidden = (jax.nn.silu(gate_value) * up_value).astype(jnp.bfloat16)
        partial_rows = jnp.dot(hidden, down, preferred_element_type=jnp.float32)
        return lax.psum_scatter(
            partial_rows.astype(jnp.bfloat16), "tp", scatter_dimension=0, tiled=True
        )

    shared = hidden_layer(everyone, shared_gate_weight, shared_up_weight, shared_down_weight)
    routed_rows = []
    for j in range(expert_local):
        rows = gathered(arrived[:, j].reshape(sp_count * capacity, model_width))
        out = hidden_layer(
            rows, expert_gate_weight[j], expert_up_weight[j], expert_down_weight[j]
        )
        routed_rows.append(out.reshape(sp_count, 1, capacity, model_width))
    routed_rows = jnp.concatenate(routed_rows, axis=1)
    returned = lax.all_to_all(routed_rows, "sp", split_axis=0, concat_axis=0, tiled=True)
    routed = jnp.dot(
        weighting, returned.reshape(slot_total, model_width).astype(jnp.float32), precision=highest
    )
    return (residual + shared.astype(jnp.float32) + routed).astype(jnp.bfloat16)


def solution(mesh):
    return jax.shard_map(
        body,
        mesh=mesh,
        in_specs=(
            P(("sp", "tp"), None),
            P("sp", "tp"),
            P("sp", "tp"),
            P("sp", "tp"),
            P("sp", "tp"),
            P("sp", "tp"),
            P("sp", "tp"),
            P("tp"),
            P("tp", None),
            P(),
            P(("sp", "tp"), None),
            P(("sp", "tp"), None),
            P("sp", None, "tp"),
            P("sp", None, "tp"),
            P("sp", "tp", None),
            P(None, "tp"),
            P(None, "tp"),
            P("tp", None),
        ),
        out_specs=P(("sp", "tp"), None),
        check_vma=False,
    )
```
